256 devices in a mesh: ep: 16 (over y, x), tp: 16 (over z, core).
Axes of the slice: x: 4, y: 4, z: 8, core: 2. Of those that a mesh axis runs over, the one named last changes fastest.
Arguments:
- query_rows: bfloat16 [2048, 2048], P('ep', 'tp'), may hold values from -32 to 32
- key_rows: bfloat16 [2048, 2048], P('ep', 'tp'), may hold values from -8 to 8
- value_rows: bfloat16 [2048, 2048], P('ep', 'tp'), may hold values from -8 to 8
- query_norm_gain: float32 [64], replicated, may hold values from 0.1 to 1.9
- key_gain: float32 [64], replicated, may hold values from 0.1 to 1.9
- break_offset: float32 [32], P('tp'), may hold values from -12 to 3
- mixer_out_weight: bfloat16 [2048, 2048], P('tp'), may hold values from -0.75 to 0.75
- routed_tokens: bfloat16 [32768, 2048], P(('ep', 'tp')), may hold values from -6 to 6
- expert_gain: float32 [2048], replicated, may hold values from 0.1 to 1.9
- routes: int32 [32768, 2], P(('ep', 'tp')), may hold values from 0 to 15, as said below
- route_scores: float32 [32768, 2], P(('ep', 'tp')), may hold values from -6 to 6
- gate_weight: bfloat16 [16, 2048, 3584], P('ep', None, 'tp'), may hold values from -0.125 to 0.125
- up_weight: bfloat16 [16, 2048, 3584], P('ep', None, 'tp'), may hold values from -0.125 to 0.125
- down_weight: bfloat16 [16, 3584, 2048], P('ep', 'tp'), may hold values from -0.09375 to 0.09375
Outputs:
- attention_output: bfloat16 [2048, 2048], P(('ep', 'tp'))
- expert_output: bfloat16 [32768, 2048], P(('ep', 'tp'))
The draws below stay inside these ranges and needn't reach their ends.
Inputs may be any that keep to these rules, and one draw needn't show every extreme that they name: `routes`: each row names 2 different experts. Among the rows of one device no expert is named more than 16 times, and one expert is named exactly 16 times by the rows of every device.
All inputs are finite; a program needn't handle non-finite values.
Results may differ from the reference program's by a relative error of at most 0.018.
Values may be sent and summed in bfloat16 or wider, within the bound.
A program may use at most 128 MiB of HBM per device.

```python
import math
import jax
import jax.numpy as jnp
from jax import lax

D = 2048
HEADS = 32
HEAD_DIM = 64
FFE = 3584
TOP_K = 2
TOK_DEV = 128
SEG = 128
SEQUENCE_TOKENS = 2048
ROUTED = 32768
EXPERTS = 16
CAP = 16
N_TP = 16


def head_axes(key):
    sample = jax.random.normal(jax.random.fold_in(key, 101), (HEADS, HEAD_DIM), jnp.float32)
    return sample * lax.rsqrt(jnp.mean(sample * sample, axis=1, keepdims=True))


def draw_query_rows(key, part):
    direction = head_axes(key)
    jitter = jax.random.normal(jax.random.fold_in(key, 1), (SEQUENCE_TOKENS, HEADS, HEAD_DIM), jnp.float32)
    rows_out = jnp.clip(0.5 * jitter + direction[None], -32.0, 32.0)
    return rows_out.reshape(SEQUENCE_TOKENS, HEADS * HEAD_DIM).astype(jnp.bfloat16)


def draw_key_rows(key, part):
    direction = head_axes(key)
    blocks_count = SEQUENCE_TOKENS // SEG
    token_position = jnp.arange(SEQUENCE_TOKENS)
    jitter = jax.random.normal(jax.random.fold_in(key, 3), (SEQUENCE_TOKENS, HEADS, HEAD_DIM), jnp.float32)
    low_end = 0.4
    high_end = 1.6
    factor = jnp.exp(jax.random.uniform(jax.random.fold_in(key, 4), (blocks_count,), jnp.float32, jnp.log(low_end), jnp.log(high_end)))
    spread = jax.random.uniform(jax.random.fold_in(key, 5), (SEQUENCE_TOKENS, HEADS), jnp.float32, 0.6, 1.4)
    toward = -factor[token_position // SEG][:, None] * spread
    micro_batches = jax.random.randint(jax.random.fold_in(key, 6), (4,), 0, SEQUENCE_TOKENS)
    broken_stick = jnp.any(token_position[:, None] == micro_batches[None, :], axis=1)
    toward = jnp.where(broken_stick[:, None], 0.2, toward)
    rows_out = jnp.clip(0.5 * jitter + toward[:, :, None] * direction[None], -8.0, 8.0)
    return rows_out.reshape(SEQUENCE_TOKENS, HEADS * HEAD_DIM).astype(jnp.bfloat16)


def draw_value_rows(key, part):
    blocks_count = SEQUENCE_TOKENS // SEG
    levels = jax.random.uniform(jax.random.fold_in(key, 7), (blocks_count, HEADS * HEAD_DIM), jnp.float32, -1.5, 1.5)
    jitter = jax.random.normal(jax.random.fold_in(key, 8), (SEQUENCE_TOKENS, HEADS * HEAD_DIM), jnp.float32)
    rows_out = jnp.clip(jitter + jnp.repeat(levels, SEG, axis=0), -8.0, 8.0)
    return rows_out.astype(jnp.bfloat16)


def draw_break_offset(key, part):
    quick_share = 0.5
    quick = jax.random.uniform(jax.random.fold_in(key, 9), (HEADS,), jnp.float32) < quick_share
    quick_value = jax.random.uniform(jax.random.fold_in(key, 10), (HEADS,), jnp.float32, 2.0, 3.0)
    slow_value = jax.random.uniform(jax.random.fold_in(key, 11), (HEADS,), jnp.float32, 5.0, 6.0) - jnp.log(SEQUENCE_TOKENS * 1.0)
    return jnp.where(quick, quick_value, slow_value).astype(jnp.float32)


def draw_routes(key, part):
    blocks_count = ROUTED // TOK_DEV

    def one_block(block_key):
        reserve = jnp.tile(jnp.arange(1, EXPERTS, dtype=jnp.int32), CAP)
        reserve = jax.random.permutation(jax.random.fold_in(block_key, 1), reserve)
        remainder = jnp.sort(reserve[:TOK_DEV * TOP_K - CAP])
        ordered = jnp.concatenate([jnp.zeros((CAP,), jnp.int32), remainder])
        paired = ordered.reshape(TOP_K, TOK_DEV).T
        shuffle = jax.random.permutation(jax.random.fold_in(block_key, 2), TOK_DEV)
        labels = jax.random.permutation(jax.random.fold_in(block_key, 3), EXPERTS).astype(jnp.int32)
        return labels[paired[shuffle]]
    block_keys = jax.random.split(jax.random.fold_in(key, 13), blocks_count)
    chosen = jax.vmap(one_block)(block_keys).reshape(ROUTED, TOP_K)
    return chosen.astype(jnp.int32)


def block_scale(rng, extent, shards, low, largest):
    factor_of, own = 1.0, jax.random.fold_in(rng, 6)
    for position, parts in shards:
        heights = jnp.exp(jax.random.uniform(jax.random.fold_in(own, position), (parts,), jnp.float32, low / len(shards), largest / len(shards)))
        factor_of = factor_of * jnp.repeat(heights, extent[position] // parts).reshape([-1 if axis == position else 1 for axis in range(len(extent))])
    return factor_of


def noise(rng, dims, deviation, reach, cuts=(), held_as=jnp.bfloat16):
    values = jax.random.normal(rng, dims, jnp.float32) * deviation
    if len(cuts) > 0:
        values = block_scale(rng, dims, cuts, -0.22, 0.18) * values
    return jnp.clip(values, min=-reach, max=reach).astype(held_as)


def setup_inputs(seed: int = 0) -> dict:
    key_list = jax.random.split(jax.random.key(seed), 15)
    return {
        "query_rows": draw_query_rows(jax.random.fold_in(key_list[14], 71), 0),
        "key_rows": draw_key_rows(jax.random.fold_in(key_list[14], 71), 0),
        "value_rows": draw_value_rows(jax.random.fold_in(key_list[14], 71), 0),
        "query_norm_gain": jnp.clip(1.0 + 0.18 * jax.random.normal(key_list[3], (HEAD_DIM,), jnp.float32), 0.1, 1.9),
        "key_gain": jnp.clip(1.0 + 0.18 * jax.random.normal(key_list[4], (HEAD_DIM,), jnp.float32), 0.1, 1.9),
        "break_offset": draw_break_offset(jax.random.fold_in(key_list[14], 71), 0),
        "mixer_out_weight": noise(key_list[6], (HEADS * HEAD_DIM, D), HEAD_DIM ** -0.5, 0.75, ((0, 16),)),
        "routed_tokens": noise(key_list[7], (ROUTED, D), 1.0, 6.0, ((0, 256),)),
        "expert_gain": jnp.clip(1.0 + 0.18 * jax.random.normal(key_list[8], (D,), jnp.float32), 0.1, 1.9),
        "routes": draw_routes(jax.random.fold_in(key_list[14], 71), 0),
        "route_scores": noise(key_list[10], (ROUTED, TOP_K), 1.5, 6.0, ((0, 256),), jnp.float32),
        "gate_weight": noise(key_list[11], (EXPERTS, D, FFE), D ** -0.5, 0.125, ((0, 16), (2, 16))),
        "up_weight": noise(key_list[12], (EXPERTS, D, FFE), D ** -0.5, 0.125, ((0, 16), (2, 16))),
        "down_weight": noise(key_list[13], (EXPERTS, FFE, D), FFE ** -0.5, 0.09375, ((0, 16), (1, 16))),
    }


EPS = 1e-06

def norm_heads(flat, gain):
    count = flat.shape[0]
    split = flat.astype(jnp.float32).reshape(count, -1, HEAD_DIM)
    scaled = split * lax.rsqrt(lax.optimization_barrier(jnp.mean(split * split, axis=2, keepdims=True)) + EPS)
    return (scaled * gain).astype(jnp.bfloat16)

def attention_part(query_rows, key_rows, value_rows, query_norm_gain, key_gain, break_offset, mixer_out_weight):
    length = query_rows.shape[0]
    query_norm = norm_heads(query_rows, query_norm_gain)
    key_norm = norm_heads(key_rows, key_gain)
    value_heads = value_rows.reshape(length, HEADS, HEAD_DIM)
    block_size = math.gcd(512, length)
    gathered = []
    for block_start in range(0, length, block_size):
        block_end = block_start + block_size
        query_place = block_start + jnp.arange(block_size, dtype=jnp.int32)[:, None]
        key_place = jnp.arange(block_end, dtype=jnp.int32)[None, :]
        before = key_place < query_place

        def one_head(inputs):
            query_head, key_head, value_head, offset_value = inputs
            scores = jnp.dot(query_head, key_head.T, preferred_element_type=jnp.float32) * HEAD_DIM ** (-0.5) + offset_value
            log_rise = jax.nn.log_sigmoid(scores)
            log_fail = jnp.where(before, log_rise - scores, 0.0)
            log_after = lax.cumsum(log_fail, axis=1, reverse=True) - log_fail
            weights = jnp.where(before, jnp.exp(log_rise + log_after), 0.0).astype(jnp.bfloat16)
            return jnp.dot(weights, value_head, preferred_element_type=jnp.float32).astype(jnp.bfloat16)
        heads_out = lax.map(one_head, (jnp.moveaxis(query_norm[block_start:block_end], 1, 0), jnp.moveaxis(key_norm[:block_end], 1, 0), jnp.moveaxis(value_heads[:block_end], 1, 0), break_offset))
        gathered.append(jnp.moveaxis(heads_out, 0, 1).reshape(block_size, HEADS * HEAD_DIM))
    heads_mixed = jnp.concatenate(gathered, axis=0)
    group_width = HEADS * HEAD_DIM // N_TP
    running_sum = jnp.zeros((length, D), jnp.float32)
    for group_index in range(N_TP):
        low_edge = group_index * group_width
        term = jnp.dot(heads_mixed[:, low_edge:low_edge + group_width], mixer_out_weight[low_edge:low_edge + group_width], preferred_element_type=jnp.float32).astype(jnp.bfloat16)
        running_sum = running_sum + term.astype(jnp.float32)
    return running_sum.astype(jnp.bfloat16)

def expert_part(routed_tokens, expert_gain, routes, route_scores, gate_weight, up_weight, down_weight):
    row_count = routed_tokens.shape[0]
    as_float = routed_tokens.astype(jnp.float32)
    normed = (as_float * lax.rsqrt(lax.optimization_barrier(jnp.mean(as_float * as_float, axis=1, keepdims=True)) + EPS) * expert_gain).astype(jnp.bfloat16)
    differences = route_scores[:, None, :] - route_scores[:, :, None]
    route_weight = 1.0 / lax.optimization_barrier(jnp.sum(jnp.exp(differences), axis=2))
    flat_routes = routes.reshape(-1).astype(jnp.int32)
    copy_count = flat_routes.shape[0]
    block_count = row_count // TOK_DEV
    member = (flat_routes[:, None] == jnp.arange(EXPERTS, dtype=jnp.int32)[None, :]).astype(jnp.int32)
    member = member.reshape(block_count, TOK_DEV * TOP_K, EXPERTS)
    ahead = lax.optimization_barrier(jnp.sum((jnp.cumsum(member, axis=1) - member) * member, axis=2)).reshape(-1)
    owner = jnp.arange(copy_count, dtype=jnp.int32) // (TOK_DEV * TOP_K)
    slot_index = (owner * CAP + ahead).astype(jnp.int32)
    sources = jnp.repeat(normed, TOP_K, axis=0)
    room = block_count * CAP
    unit_width = FFE // N_TP

    def single_expert(carry, expert_index):
        chosen = flat_routes == expert_index
        target = jnp.where(chosen, slot_index, room).astype(jnp.int32)
        rows_in = jnp.zeros((room, D), jnp.bfloat16).at[target].set(sources, mode='drop')
        gate_part = jnp.dot(rows_in, gate_weight[expert_index], preferred_element_type=jnp.float32)
        up_part = jnp.dot(rows_in, up_weight[expert_index], preferred_element_type=jnp.float32)
        hidden = (jax.nn.silu(gate_part) * up_part).astype(jnp.bfloat16)
        down_here = down_weight[expert_index]
        running_sum = jnp.zeros((room, D), jnp.float32)
        for unit_index in range(N_TP):
            low_edge = unit_index * unit_width
            term = jnp.dot(hidden[:, low_edge:low_edge + unit_width], down_here[low_edge:low_edge + unit_width], preferred_element_type=jnp.float32).astype(jnp.bfloat16)
            running_sum = running_sum + term.astype(jnp.float32)
        result = running_sum.astype(jnp.bfloat16)
        picked = result[jnp.minimum(target, room - 1)]
        return (jnp.where(chosen[:, None], picked.astype(jnp.float32), carry), None)
    results, _ = lax.scan(single_expert, jnp.zeros((copy_count, D), jnp.float32), jnp.arange(EXPERTS, dtype=jnp.int32))
    results = results.reshape(row_count, TOP_K, D)
    return lax.optimization_barrier(jnp.sum(route_weight[..., None] * results, axis=1)).astype(jnp.bfloat16)

def reference(query_rows, key_rows, value_rows, query_norm_gain, key_gain, break_offset, mixer_out_weight, routed_tokens, expert_gain, routes, route_scores, gate_weight, up_weight, down_weight):
    attention_output = attention_part(query_rows, key_rows, value_rows, query_norm_gain, key_gain, break_offset, mixer_out_weight)
    expert_output = expert_part(routed_tokens, expert_gain, routes, route_scores, gate_weight, up_weight, down_weight)
    return (attention_output, expert_output)
```

```python
import functools

import jax
import jax.numpy as jnp
from jax import lax
from jax.experimental import pallas as pl
from jax.experimental.pallas import tpu as pltpu
from jax.sharding import PartitionSpec as P

HEAD_DIM = 64
EPS = 1e-06
MESH = pl.DeviceIdType.MESH
EP = 16
NZ = 8
CAP = 16
HALF = EP // 2
F32 = jnp.float32
BF16 = jnp.bfloat16


def iota(shape, dim):
    return lax.broadcasted_iota(jnp.int32, shape, dim)


def kernel(
    query_ref,
    key_ref,
    value_ref,
    query_gain_ref,
    key_gain_ref,
    offset_ref,
    mixer_hbm,
    tokens_ref,
    expert_gain_ref,
    routes_ref,
    scores_ref,
    gate_hbm,
    up_hbm,
    down_hbm,
    attn_out,
    expert_out,
    gate_w,
    up_w,
    down_w,
    mixer_w,
    kv,
    tok,
    slots,
    outgoing,
    arrived,
    terms,
    ring_out,
    ring_in,
    returned,
    mix_mine,
    mix_theirs,
    mix_out,
    mix_in,
    load_sem,
    pair_send,
    pair_recv,
    kv_send,
    kv_recv,
    up_send,
    up_recv,
    dn_send,
    dn_recv,
    slot_send,
    slot_recv,
    disp_send,
    disp_recv,
    ring_send,
    ring_recv,
    ret_send,
    ret_recv,
    mix_send,
    mix_recv,
):
    ep = lax.axis_index("ep")
    tp = lax.axis_index("tp")
    z, core = tp // 2, tp % 2
    above = (ep, lax.rem(z + 1, NZ) * 2 + core)
    below = (ep, lax.rem(z + NZ - 1, NZ) * 2 + core)
    sibling = (ep, z * 2 + 1 - core)
    rows = query_ref.shape[0]
    tokens, width = tokens_ref.shape

    def remote(src, dst, send, recv, device):
        return pltpu.make_async_remote_copy(
            src_ref=src,
            dst_ref=dst,
            send_sem=send,
            recv_sem=recv,
            device_id=device,
            device_id_type=MESH,
        )

    barrier = pltpu.get_barrier_semaphore()

    def greet_ep(j, _):
        pl.semaphore_signal(
            barrier, inc=1, device_id=(lax.rem(ep + j, EP), tp), device_id_type=MESH
        )
        return 0

    def greet_z(j, _):
        pl.semaphore_signal(
            barrier,
            inc=1,
            device_id=(ep, lax.rem(z + j, NZ) * 2 + core),
            device_id_type=MESH,
        )
        return 0

    lax.fori_loop(1, EP, greet_ep, 0)
    lax.fori_loop(1, NZ, greet_z, 0)
    pl.semaphore_signal(barrier, inc=1, device_id=sibling, device_id_type=MESH)

    weights = ((gate_hbm, gate_w), (up_hbm, up_w), (down_hbm, down_w), (mixer_hbm, mixer_w))
    loads = [
        pltpu.make_async_copy(src, dst.at[0], load_sem.at[i])
        for i, (src, dst) in enumerate(weights)
    ]
    for copy in loads:
        copy.start()

    lane = iota((rows, 128), 1)
    first_head = lane < HEAD_DIM

    def norm_heads(flat, gain):
        split = flat.astype(F32)
        squares = split * split
        mean_a = jnp.sum(jnp.where(first_head, squares, 0.0), axis=1, keepdims=True) / HEAD_DIM
        mean_b = jnp.sum(jnp.where(first_head, 0.0, squares), axis=1, keepdims=True) / HEAD_DIM
        scale = jnp.where(first_head, lax.rsqrt(mean_a + EPS), lax.rsqrt(mean_b + EPS))
        return (split * scale * gain).astype(BF16)

    key_norm = norm_heads(key_ref[...], key_gain_ref[...])
    kv[ep, 0] = key_norm
    kv[ep, 1] = value_ref[...]

    as_float = tokens_ref[...].astype(F32)
    mean = jnp.mean(as_float * as_float, axis=1, keepdims=True)
    tok[0] = (as_float * lax.rsqrt(mean + EPS) * expert_gain_ref[...]).astype(BF16)

    expert_lane = iota((tokens, 128), 1)
    route_a, route_b = routes_ref[:, 0:1], routes_ref[:, 1:2]
    member_a = jnp.where(route_a == expert_lane, 1.0, 0.0).astype(F32)
    member_b = jnp.where(route_b == expert_lane, 1.0, 0.0).astype(F32)
    lower = jnp.where(iota((tokens, tokens), 1) < iota((tokens, tokens), 0), 1.0, 0.0).astype(BF16)
    ahead_a = jnp.dot(lower, member_a.astype(BF16), preferred_element_type=F32)
    ahead_b = jnp.dot(lower, member_b.astype(BF16), preferred_element_type=F32)
    ahead_b = ahead_b + jnp.sum(member_a, axis=0, keepdims=True)
    expert_base = (expert_lane * CAP).astype(F32)
    slot_a = jnp.sum(member_a * (ahead_a + expert_base), axis=1, keepdims=True)
    slot_b = jnp.sum(member_b * (ahead_b + expert_base), axis=1, keepdims=True)
    slots[0, 0] = jnp.transpose(jnp.broadcast_to(slot_a, (tokens, 128)))[0:8]
    slots[0, 1] = jnp.transpose(jnp.broadcast_to(slot_b, (tokens, 128)))[0:8]

    pl.semaphore_wait(barrier, EP - 1 + NZ - 1 + 1)

    def ag_up(hop):
        return remote(tok.at[hop - 1], tok.at[hop], up_send.at[hop], up_recv.at[hop], above)

    def ag_down(hop):
        return remote(
            tok.at[lax.rem(NZ + 1 - hop, NZ)],
            tok.at[NZ - hop],
            dn_send.at[hop],
            dn_recv.at[hop],
            below,
        )

    half_tok = tokens // 2

    def last_up():
        part = pl.ds(0, half_tok)
        return remote(tok.at[3, part], tok.at[4, part], up_send.at[4], up_recv.at[4], above)

    def last_down():
        part = pl.ds(half_tok, half_tok)
        return remote(tok.at[5, part], tok.at[4, part], dn_send.at[4], dn_recv.at[4], below)

    def slot_copy(j):
        peer = (ep, lax.rem(z + j, NZ) * 2 + core)
        return remote(slots.at[0], slots.at[j], slot_send.at[j], slot_recv.at[j], peer)

    ag_up(1).start()
    ag_down(1).start()

    def send_slots(j, _):
        slot_copy(j).start()
        return 0

    lax.fori_loop(1, NZ, send_slots, 0)

    def kv_copy(source, target):
        return remote(
            kv.at[source], kv.at[source], kv_send.at[target], kv_recv.at[source], (target, tp)
        )

    def send_kv(j, _):
        kv_copy(ep, j).start()
        return 0

    lax.fori_loop(ep + 1, EP, send_kv, 0)

    pair_copies = [
        remote(src, dst.at[1], pair_send.at[i], pair_recv.at[i], sibling)
        for i, (src, dst) in enumerate(weights)
    ]
    for copy in pair_copies:
        copy.start()

    slot_rows = iota((EP * CAP, tokens), 0).astype(F32)

    def dispatch(step, distance):
        row_a = slots[distance, 0][0:1]
        row_b = slots[distance, 1][0:1]
        pick = jnp.where((slot_rows == row_a) | (slot_rows == row_b), 1.0, 0.0).astype(BF16)
        picked = jnp.dot(pick, tok[distance], preferred_element_type=F32).astype(BF16)
        outgoing[step] = picked.reshape(EP, CAP, width)

        def send(j, _):
            peer = lax.rem(ep + j, EP)
            remote(
                outgoing.at[step, peer],
                arrived.at[step, ep],
                disp_send.at[step],
                disp_recv.at[step],
                (peer, tp),
            ).start()
            return 0

        lax.fori_loop(1, EP, send, 0)
        arrived[step, ep] = outgoing[step, ep]

    def all_but_one(buffer, send, recv):
        block = buffer.at[pl.ds(0, EP - 1)]
        return remote(block, block, send, recv, sibling)

    dispatch(0, 0)

    def wait_slots(j, _):
        slot_copy(j).wait_recv()
        return 0

    lax.fori_loop(1, NZ, wait_slots, 0)

    def advance(step):
        @pl.when(step <= 3)
        def _():
            ag_up(step).wait_recv()

            @pl.when(step <= 2)
            def _():
                ag_up(step + 1).start()

            @pl.when(step == 3)
            def _():
                last_up().start()

            ag_down(step).wait_recv()

            @pl.when(step <= 2)
            def _():
                ag_down(step + 1).start()

            @pl.when(step == 3)
            def _():
                last_down().start()

        @pl.when(step == 4)
        def _():
            last_up().wait_recv()
            last_down().wait_recv()

        dispatch(step, jnp.where(ep < HALF, step, NZ - step))

    def attention():
        query_norm = norm_heads(query_ref[...], query_gain_ref[...])
        zero = jnp.zeros_like(query_norm)
        queries = jnp.concatenate(
            [jnp.where(first_head, query_norm, zero), jnp.where(first_head, zero, query_norm)],
            axis=0,
        )
        row = iota((2 * rows, rows), 0)
        column = iota((2 * rows, rows), 1)
        offsets = jnp.where(row < rows, offset_ref[0], offset_ref[1])
        position = jnp.where(row < rows, row, row - rows)
        after = jnp.where(iota((rows, rows), 0) > iota((rows, rows), 1), 1.0, 0.0).astype(BF16)

        def absorb(j, state):
            mixed, carried = state

            @pl.when(j < ep)
            def _():
                kv_copy(j, ep).wait_recv()

            keys, values = kv[j, 0], kv[j, 1]
            scores = lax.dot_general(
                queries, keys, (((1,), (1,)), ((), ())), preferred_element_type=F32
            )
            scores = scores * HEAD_DIM ** (-0.5) + offsets
            allowed = (column < position) | (j < ep)
            log_fail = -(jnp.maximum(scores, 0.0) + jnp.log1p(jnp.exp(-jnp.abs(scores))))
            log_rise = scores + log_fail
            log_fail = jnp.where(allowed, log_fail, 0.0)
            high = log_fail.astype(BF16)
            rest = log_fail - high.astype(F32)
            middle = rest.astype(BF16)
            low = (rest - middle.astype(F32)).astype(BF16)
            between = (
                jnp.dot(high, after, preferred_element_type=F32)
                + jnp.dot(middle, after, preferred_element_type=F32)
                + jnp.dot(low, after, preferred_element_type=F32)
            )
            weights = jnp.where(allowed, jnp.exp(log_rise + between + carried), 0.0).astype(BF16)
            mixed = mixed + jnp.dot(weights, values, preferred_element_type=F32)
            carried = carried + jnp.sum(log_fail, axis=1, keepdims=True)
            return mixed, carried

        state = (jnp.zeros((2 * rows, 128), F32), jnp.zeros((2 * rows, 1), F32))
        mixed, _ = lax.fori_loop(0, ep + 1, lambda t, s: absorb(ep - t, s), state)
        heads = jnp.where(first_head, mixed[:rows], mixed[rows:]).astype(BF16)
        to_row = iota((rows, rows), 0)
        from_row = iota((rows, rows), 1)
        owner_core = to_row // 64
        within = to_row % 64
        source = (within // 8) * 16 + owner_core * 8 + within % 8
        order = jnp.where(from_row == source, 1.0, 0.0).astype(BF16)
        ordered = jnp.dot(order, heads, preferred_element_type=F32).astype(BF16)
        mix_mine[0] = ordered[:64]
        mix_mine[1] = ordered[64:]

    def mix_pair():
        return remote(
            mix_mine.at[1 - core], mix_theirs, pair_send.at[4], pair_recv.at[4], sibling
        )

    def mix_terms():
        loads[3].wait()
        pair_copies[3].wait_recv()
        mix_pair().wait_recv()
        term = jnp.dot(mix_mine[core], mixer_w[0], preferred_element_type=F32)
        term = term + jnp.dot(mix_theirs[...], mixer_w[1], preferred_element_type=F32)
        for i in range(NZ):
            mix_out[i] = term[8 * i : 8 * i + 8].astype(BF16)

        def send(j, _):
            to = lax.rem(z + j, NZ)
            remote(mix_out.at[to], mix_in.at[j], mix_send, mix_recv, (ep, to * 2 + core)).start()
            return 0

        lax.fori_loop(1, NZ, send, 0)

    def experts(step):
        rows_in = arrived[lax.rem(step, NZ)].reshape(EP * CAP, width)
        total = None
        for i in range(2):
            gate = jnp.dot(rows_in, gate_w[i], preferred_element_type=F32)
            up = jnp.dot(rows_in, up_w[i], preferred_element_type=F32)
            hidden = (gate / (1.0 + jnp.exp(-gate)) * up).astype(BF16)
            term = jnp.dot(hidden, down_w[i], preferred_element_type=F32)
            total = term if total is None else total + term
        terms[...] = total

    def ring(step, part, device):
        return remote(
            ring_out.at[step, pl.ds(part * HALF, HALF)],
            ring_in.at[step + 1, pl.ds(part * HALF, HALF)],
            ring_send.at[part, step],
            ring_recv.at[part, step + 1],
            device,
        )

    half_rows = HALF * CAP

    def combine(step):
        for part, device in ((0, above), (1, below)):
            blocks = pl.ds(part * HALF, HALF)
            mine = terms[part * half_rows : (part + 1) * half_rows, :]

            @pl.when(step == 1)
            def _():
                ring_out[step, blocks] = mine.astype(BF16).reshape(HALF, CAP, width)

            @pl.when(step >= 2)
            def _():
                ring(step - 1, part, device).wait_recv()
                sofar = ring_in[step, blocks].reshape(half_rows, width).astype(F32)
                ring_out[step, blocks] = (mine + sofar).astype(BF16).reshape(HALF, CAP, width)

            @pl.when(step < NZ)
            def _():
                ring(step, part, device).start()

            @pl.when(step == NZ)
            def _():
                def send(j, _):
                    peer = part * HALF + j

                    @pl.when(peer != ep)
                    def _():
                        remote(
                            ring_out.at[NZ, peer],
                            returned.at[ep],
                            ret_send,
                            ret_recv,
                            (peer, tp),
                        ).start()

                    return 0

                lax.fori_loop(0, HALF, send, 0)

    advance(1)
    attention()
    mix_pair().start()
    for i in range(3):
        loads[i].wait()
        pair_copies[i].wait_recv()

    def one_step(step, _):
        @pl.when(step + 1 < NZ)
        def _():
            advance(step + 1)

        every = all_but_one(
            arrived.at[lax.rem(step, NZ)], disp_send.at[0], disp_recv.at[lax.rem(step, NZ)]
        )
        every.wait_recv()
        experts(step)
        combine(step)

        @pl.when(step == 1)
        def _():
            mix_terms()

        return 0

    lax.fori_loop(1, NZ + 1, one_step, 0)
    returned[ep] = ring_out[NZ, ep]

    peers = mix_in.at[pl.ds(1, NZ - 1)]
    remote(peers, peers, mix_send, mix_recv, sibling).wait()
    total = mix_out[z].astype(F32)
    for j in range(1, NZ):
        total = total + mix_in[j].astype(F32)
    attn_out[...] = total.astype(BF16)

    slot_lane = iota((tokens, EP * CAP), 1).astype(F32)
    select_a = jnp.where(slot_lane == slot_a, 1.0, 0.0).astype(BF16)
    select_b = jnp.where(slot_lane == slot_b, 1.0, 0.0).astype(BF16)
    score_a, score_b = scores_ref[:, 0:1], scores_ref[:, 1:2]
    weight_a = 1.0 / (1.0 + jnp.exp(score_b - score_a))
    weight_b = 1.0 / (jnp.exp(score_a - score_b) + 1.0)
    all_but_one(returned, ret_send, ret_recv).wait()
    results = returned[...].reshape(EP * CAP, width)
    result_a = jnp.dot(select_a, results, preferred_element_type=F32)
    result_b = jnp.dot(select_b, results, preferred_element_type=F32)
    expert_out[...] = (weight_a * result_a + weight_b * result_b).astype(BF16)

    for hop in range(1, 4):
        ag_up(hop).wait_send()
        ag_down(hop).wait_send()
    last_up().wait_send()
    last_down().wait_send()
    mix_pair().wait_send()
    for copy in pair_copies:
        copy.wait_send()

    def drain_slots(j, _):
        slot_copy(j).wait_send()
        return 0

    lax.fori_loop(1, NZ, drain_slots, 0)

    def drain_kv(j, _):
        kv_copy(ep, j).wait_send()
        return 0

    lax.fori_loop(ep + 1, EP, drain_kv, 0)

    def drain_dispatch(step, _):
        all_but_one(outgoing.at[step], disp_send.at[step], disp_recv.at[step]).wait_send()
        return 0

    lax.fori_loop(0, NZ, drain_dispatch, 0)

    def drain_ring(step, _):
        ring(step, 0, above).wait_send()
        ring(step, 1, below).wait_send()
        return 0

    lax.fori_loop(1, NZ, drain_ring, 0)


def body(
    query_rows,
    key_rows,
    value_rows,
    query_norm_gain,
    key_gain,
    break_offset,
    mixer_out_weight,
    routed_tokens,
    expert_gain,
    routes,
    route_scores,
    gate_weight,
    up_weight,
    down_weight,
):
    rows = query_rows.shape[0]
    tokens, width = routed_tokens.shape
    units = gate_weight.shape[2]
    vmem = pl.BlockSpec(memory_space=pltpu.VMEM)
    smem = pl.BlockSpec(memory_space=pltpu.SMEM)
    hbm = pl.BlockSpec(memory_space=pl.ANY)
    dma = pltpu.SemaphoreType.DMA
    return pl.pallas_call(
        kernel,
        out_shape=(
            jax.ShapeDtypeStruct((rows // (2 * NZ), width), BF16),
            jax.ShapeDtypeStruct((tokens, width), BF16),
        ),
        in_specs=[vmem] * 5 + [smem, hbm] + [vmem] * 4 + [hbm] * 3,
        out_specs=(vmem, vmem),
        scratch_shapes=[
            pltpu.VMEM((2, width, units), BF16),
            pltpu.VMEM((2, width, units), BF16),
            pltpu.VMEM((2, units, width), BF16),
            pltpu.VMEM((2, 128, width), BF16),
            pltpu.VMEM((EP, 2, rows, 128), BF16),
            pltpu.VMEM((NZ, tokens, width), BF16),
            pltpu.VMEM((NZ, 2, 8, 128), F32),
            pltpu.VMEM((NZ, EP, CAP, width), BF16),
            pltpu.VMEM((NZ, EP, CAP, width), BF16),
            pltpu.VMEM((EP * CAP, width), F32),
            pltpu.VMEM((NZ + 1, EP, CAP, width), BF16),
            pltpu.VMEM((NZ + 1, EP, CAP, width), BF16),
            pltpu.VMEM((EP, CAP, width), BF16),
            pltpu.VMEM((2, 64, 128), BF16),
            pltpu.VMEM((64, 128), BF16),
            pltpu.VMEM((NZ, 8, width), BF16),
            pltpu.VMEM((NZ, 8, width), BF16),
            dma((4,)),
            dma((5,)),
            dma((5,)),
            dma((EP,)),
            dma((EP,)),
            dma((5,)),
            dma((5,)),
            dma((5,)),
            dma((5,)),
            dma((NZ,)),
            dma((NZ,)),
            dma((NZ,)),
            dma((NZ,)),
            dma((2, NZ + 1)),
            dma((2, NZ + 1)),
            dma,
            dma,
            dma,
            dma,
        ],
        compiler_params=pltpu.CompilerParams(
            collective_id=0, has_side_effects=True, vmem_limit_bytes=67043328
        ),
    )(
        query_rows,
        key_rows,
        value_rows,
        jnp.tile(query_norm_gain, 2)[None, :],
        jnp.tile(key_gain, 2)[None, :],
        break_offset,
        mixer_out_weight,
        routed_tokens,
        expert_gain[None, :],
        routes,
        route_scores,
        gate_weight[0],
        up_weight[0],
        down_weight[0],
    )


def solution(mesh):
    in_specs = (
        P("ep", "tp"),
        P("ep", "tp"),
        P("ep", "tp"),
        P(),
        P(),
        P("tp"),
        P("tp", None),
        P(("ep", "tp"), None),
        P(),
        P(("ep", "tp"), None),
        P(("ep", "tp"), None),
        P("ep", None, "tp"),
        P("ep", None, "tp"),
        P("ep", "tp", None),
    )
    out_specs = (P(("ep", "tp"), None), P(("ep", "tp"), None))
    return jax.shard_map(body, mesh=mesh, in_specs=in_specs, out_specs=out_specs, check_vma=False)
```

```python
import functools

import jax
import jax.numpy as jnp
from jax import lax
from jax.experimental import pallas as pl
from jax.experimental.pallas import tpu as pltpu
from jax.sharding import PartitionSpec as P

HEAD_DIM = 64
EPS = 1e-06
MESH = pl.DeviceIdType.MESH
EP = 16
NZ = 8
CAP = 16
HALF = EP // 2
F32 = jnp.float32
BF16 = jnp.bfloat16


def iota(shape, dim):
    return lax.broadcasted_iota(jnp.int32, shape, dim)


def kernel(
    query_ref,
    key_ref,
    value_ref,
    query_gain_ref,
    key_gain_ref,
    offset_ref,
    mixer_hbm,
    tokens_ref,
    expert_gain_ref,
    routes_ref,
    scores_ref,
    gate_hbm,
    up_hbm,
    down_hbm,
    attn_out,
    expert_out,
    gate_w,
    up_w,
    down_w,
    mixer_w,
    kv,
    tok,
    slots,
    outgoing,
    arrived,
    terms,
    ring_out,
    ring_in,
    returned,
    mix_mine,
    mix_theirs,
    mix_out,
    mix_in,
    load_sem,
    pair_send,
    pair_recv,
    kv_send,
    kv_recv,
    up_send,
    up_recv,
    dn_send,
    dn_recv,
    slot_send,
    slot_recv,
    disp_send,
    disp_recv,
    ring_send,
    ring_recv,
    ret_send,
    ret_recv,
    mix_send,
    mix_recv,
):
    ep = lax.axis_index("ep")
    tp = lax.axis_index("tp")
    z, core = tp // 2, tp % 2
    above = (ep, lax.rem(z + 1, NZ) * 2 + core)
    below = (ep, lax.rem(z + NZ - 1, NZ) * 2 + core)
    sibling = (ep, z * 2 + 1 - core)
    rows = query_ref.shape[0]
    tokens, width = tokens_ref.shape
    position_here = lax.rem(ep // 4 + ep % 4, 4) * 4 + ep // 4
    goes_up = position_here < HALF

    def at_position(place):
        return place % 4 * 4 + lax.rem(place // 4 + 4 - place % 4, 4)

    def remote(src, dst, send, recv, device):
        return pltpu.make_async_remote_copy(
            src_ref=src,
            dst_ref=dst,
            send_sem=send,
            recv_sem=recv,
            device_id=device,
            device_id_type=MESH,
        )

    barrier = pltpu.get_barrier_semaphore()

    def greet_ep(j, _):
        pl.semaphore_signal(
            barrier, inc=1, device_id=(lax.rem(ep + j, EP), tp), device_id_type=MESH
        )
        return 0

    def greet_z(j, _):
        pl.semaphore_signal(
            barrier,
            inc=1,
            device_id=(ep, lax.rem(z + j, NZ) * 2 + core),
            device_id_type=MESH,
        )
        return 0

    lax.fori_loop(1, EP, greet_ep, 0)
    lax.fori_loop(1, NZ, greet_z, 0)
    pl.semaphore_signal(barrier, inc=1, device_id=sibling, device_id_type=MESH)

    weights = ((gate_hbm, gate_w), (up_hbm, up_w), (down_hbm, down_w), (mixer_hbm, mixer_w))
    loads = [
        pltpu.make_async_copy(src, dst.at[0], load_sem.at[i])
        for i, (src, dst) in enumerate(weights)
    ]
    for copy in loads:
        copy.start()

    lane = iota((rows, 128), 1)
    first_head = lane < HEAD_DIM

    def norm_heads(flat, gain):
        split = flat.astype(F32)
        squares = split * split
        mean_a = jnp.sum(jnp.where(first_head, squares, 0.0), axis=1, keepdims=True) / HEAD_DIM
        mean_b = jnp.sum(jnp.where(first_head, 0.0, squares), axis=1, keepdims=True) / HEAD_DIM
        scale = jnp.where(first_head, lax.rsqrt(mean_a + EPS), lax.rsqrt(mean_b + EPS))
        return (split * scale * jnp.concatenate([gain, gain], axis=1)).astype(BF16)

    key_norm = norm_heads(key_ref[...], key_gain_ref[...])
    kv[ep, 0] = key_norm
    kv[ep, 1] = value_ref[...]

    as_float = tokens_ref[...].astype(F32)
    mean = jnp.mean(as_float * as_float, axis=1, keepdims=True)
    tok[0] = (as_float * lax.rsqrt(mean + EPS) * expert_gain_ref[...]).astype(BF16)

    expert_row = iota((EP, tokens), 0)
    member_a = jnp.where(routes_ref[0:1, :] == expert_row, 1.0, 0.0).astype(F32)
    member_b = jnp.where(routes_ref[1:2, :] == expert_row, 1.0, 0.0).astype(F32)
    earlier = jnp.where(iota((tokens, tokens), 0) < iota((tokens, tokens), 1), 1.0, 0.0)
    earlier = earlier.astype(BF16)
    ahead_a = jnp.dot(member_a.astype(BF16), earlier, preferred_element_type=F32)
    ahead_b = jnp.dot(member_b.astype(BF16), earlier, preferred_element_type=F32)
    ahead_b = ahead_b + jnp.sum(member_a, axis=1, keepdims=True)
    expert_base = (expert_row * CAP).astype(F32)
    slot_a = jnp.sum(member_a * (ahead_a + expert_base), axis=0, keepdims=True)
    slot_b = jnp.sum(member_b * (ahead_b + expert_base), axis=0, keepdims=True)
    slots[0, 0] = jnp.broadcast_to(slot_a, (8, tokens))
    slots[0, 1] = jnp.broadcast_to(slot_b, (8, tokens))

    with jax.named_scope("wait_entry"):
        pl.semaphore_wait(barrier, EP - 1 + NZ - 1 + 1)

    part_tok = tokens // 2

    def ag_up(hop, chunk):
        part = pl.ds(chunk * part_tok, part_tok)
        return remote(
            tok.at[hop - 1, part],
            tok.at[hop, part],
            up_send.at[chunk, hop],
            up_recv.at[chunk, hop],
            above,
        )

    def ag_down(hop, chunk):
        part = pl.ds(chunk * part_tok, part_tok)
        return remote(
            tok.at[lax.rem(NZ + 1 - hop, NZ), part],
            tok.at[NZ - hop, part],
            dn_send.at[chunk, hop],
            dn_recv.at[chunk, hop],
            below,
        )

    def slot_copy(j):
        peer = (ep, lax.rem(z + j, NZ) * 2 + core)
        return remote(slots.at[0], slots.at[j], slot_send.at[j], slot_recv.at[j], peer)

    def send_slots(j, _):
        slot_copy(j).start()
        return 0

    lax.fori_loop(1, NZ, send_slots, 0)
    for chunk in range(2):
        ag_up(1, chunk).start()
        ag_down(1, chunk).start()

    def kv_copy(source, target):
        return remote(
            kv.at[source], kv.at[source], kv_send.at[target], kv_recv.at[source], (target, tp)
        )

    def send_kv(j, _):
        kv_copy(ep, j).start()
        return 0

    lax.fori_loop(ep + 1, EP, send_kv, 0)

    pair_copies = [
        remote(src, dst.at[1], pair_send.at[i], pair_recv.at[i], sibling)
        for i, (src, dst) in enumerate(weights)
    ]
    for copy in pair_copies:
        copy.start()

    slot_rows = iota((EP * CAP, tokens), 0).astype(F32)

    def dispatch(step, distance):
        row_a = slots[distance, 0][0:1]
        row_b = slots[distance, 1][0:1]
        pick = jnp.where((slot_rows == row_a) | (slot_rows == row_b), 1.0, 0.0).astype(BF16)
        picked = jnp.dot(pick, tok[distance], preferred_element_type=F32).astype(BF16)
        outgoing[step] = picked.reshape(EP, CAP, width)

        def send(j, _):
            peer = lax.rem(ep + j, EP)
            remote(
                outgoing.at[step, peer],
                arrived.at[step, position_here],
                disp_send.at[step],
                disp_recv.at[step],
                (peer, tp),
            ).start()
            return 0

        lax.fori_loop(1, EP, send, 0)
        arrived[step, position_here] = outgoing[step, ep]

    def all_but_one(buffer, send, recv):
        block = buffer.at[pl.ds(0, EP - 1)]
        return remote(block, block, send, recv, sibling)

    def wait_slots(j, _):
        slot_copy(j).wait_recv()
        return 0

    def advance(step):
        @pl.when(step <= 3)
        def _():
            for chunk in range(2):
                with jax.named_scope("wait_up"):
                    ag_up(step, chunk).wait_recv()

                @pl.when(step <= 3 - chunk)
                def _():
                    ag_up(step + 1, chunk).start()

                with jax.named_scope("wait_down"):
                    ag_down(step, chunk).wait_recv()

                @pl.when(step <= 2 + chunk)
                def _():
                    ag_down(step + 1, chunk).start()

        @pl.when(step == 4)
        def _():
            with jax.named_scope("wait_last"):
                ag_up(4, 0).wait_recv()
                ag_down(4, 1).wait_recv()

        @pl.when(step == 1)
        def _():
            with jax.named_scope("wait_slots"):
                lax.fori_loop(1, NZ, wait_slots, 0)

        with jax.named_scope("dispatch"):
            distance = lax.rem(jnp.where(goes_up, step, NZ - step), NZ)
            dispatch(lax.rem(step, NZ), distance)

    def attention():
        query_norm = norm_heads(query_ref[...], query_gain_ref[...])
        zero = jnp.zeros_like(query_norm)
        queries = jnp.concatenate(
            [jnp.where(first_head, query_norm, zero), jnp.where(first_head, zero, query_norm)],
            axis=0,
        )
        row = iota((2 * rows, rows), 0)
        column = iota((2 * rows, rows), 1)
        offsets = jnp.where(row < rows, offset_ref[0], offset_ref[1])
        position = jnp.where(row < rows, row, row - rows)
        after = jnp.where(iota((rows, rows), 0) > iota((rows, rows), 1), 1.0, 0.0).astype(BF16)

        def absorb(j, state):
            mixed, carried = state

            @pl.when(j < ep)
            def _():
                kv_copy(j, ep).wait_recv()

            keys, values = kv[j, 0], kv[j, 1]
            scores = lax.dot_general(
                queries, keys, (((1,), (1,)), ((), ())), preferred_element_type=F32
            )
            scores = scores * HEAD_DIM ** (-0.5) + offsets
            allowed = (column < position) | (j < ep)
            log_fail = -(jnp.maximum(scores, 0.0) + jnp.log1p(jnp.exp(-jnp.abs(scores))))
            log_rise = scores + log_fail
            log_fail = jnp.where(allowed, log_fail, 0.0)
            high = log_fail.astype(BF16)
            rest = log_fail - high.astype(F32)
            middle = rest.astype(BF16)
            low = (rest - middle.astype(F32)).astype(BF16)
            between = (
                jnp.dot(high, after, preferred_element_type=F32)
                + jnp.dot(middle, after, preferred_element_type=F32)
                + jnp.dot(low, after, preferred_element_type=F32)
            )
            weights = jnp.where(allowed, jnp.exp(log_rise + between + carried), 0.0).astype(BF16)
            mixed = mixed + jnp.dot(weights, values, preferred_element_type=F32)
            carried = carried + jnp.sum(log_fail, axis=1, keepdims=True)
            return mixed, carried

        state = (jnp.zeros((2 * rows, 128), F32), jnp.zeros((2 * rows, 1), F32))
        mixed, _ = lax.fori_loop(0, ep + 1, lambda t, s: absorb(ep - t, s), state)
        heads = jnp.where(first_head, mixed[:rows], mixed[rows:]).astype(BF16)
        to_row = iota((rows, rows), 0)
        from_row = iota((rows, rows), 1)
        owner_core = to_row // 64
        within = to_row % 64
        source = (within // 8) * 16 + owner_core * 8 + within % 8
        order = jnp.where(from_row == source, 1.0, 0.0).astype(BF16)
        ordered = jnp.dot(order, heads, preferred_element_type=F32).astype(BF16)
        mix_mine[0] = ordered[:64]
        mix_mine[1] = ordered[64:]

    def mix_pair():
        return remote(
            mix_mine.at[1 - core], mix_theirs, pair_send.at[4], pair_recv.at[4], sibling
        )

    def mix_terms():
        loads[3].wait()
        pair_copies[3].wait_recv()
        mix_pair().wait_recv()
        term = jnp.dot(mix_mine[core], mixer_w[0], preferred_element_type=F32)
        term = term + jnp.dot(mix_theirs[...], mixer_w[1], preferred_element_type=F32)
        for i in range(NZ):
            mix_out[i] = term[8 * i : 8 * i + 8].astype(BF16)

        def send(j, _):
            to = lax.rem(z + j, NZ)
            remote(mix_out.at[to], mix_in.at[j], mix_send, mix_recv, (ep, to * 2 + core)).start()
            return 0

        lax.fori_loop(1, NZ, send, 0)

    def experts(step):
        rows_in = arrived[lax.rem(step, NZ)].reshape(EP * CAP, width)
        across = (((1,), (1,)), ((), ()))
        units = 2 * gate_w.shape[1]
        gate = lax.dot_general(
            rows_in, gate_w[...].reshape(units, width), across, preferred_element_type=F32
        )
        up = lax.dot_general(
            rows_in, up_w[...].reshape(units, width), across, preferred_element_type=F32
        )
        hidden = (gate / (1.0 + jnp.exp(-gate)) * up).astype(BF16)
        terms[...] = jnp.dot(
            hidden, down_w[...].reshape(units, width), preferred_element_type=F32
        )

    quarter = EP // 4
    quarter_rows = quarter * CAP

    def ring(step, part, chunk):
        blocks = pl.ds((part * 2 + chunk) * quarter, quarter)
        return remote(
            ring_out.at[step, blocks],
            ring_in.at[step + 1, blocks],
            ring_send.at[part * 2 + chunk, step],
            ring_recv.at[part * 2 + chunk, step + 1],
            (above, below)[part],
        )

    def combine(step):
        for chunk in range(2):
            for part in range(2):
                first = (part * 2 + chunk) * quarter
                blocks = pl.ds(first, quarter)
                mine = terms[first * CAP : (first + quarter) * CAP, :]

                @pl.when(step == 1)
                def _():
                    ring_out[step, blocks] = mine.astype(BF16).reshape(quarter, CAP, width)

                @pl.when(step >= 2)
                def _():
                    with jax.named_scope("wait_ring"):
                        ring(step - 1, part, chunk).wait_recv()
                    sofar = ring_in[step, blocks].reshape(quarter_rows, width).astype(F32)
                    total = (mine + sofar).astype(BF16)
                    ring_out[step, blocks] = total.reshape(quarter, CAP, width)

                @pl.when(step < NZ)
                def _():
                    ring(step, part, chunk).start()

                @pl.when(step == NZ)
                def _():
                    def send(j, _):
                        peer = at_position(first + j)

                        @pl.when(peer != ep)
                        def _():
                            remote(
                                ring_out.at[NZ, first + j],
                                returned.at[ep],
                                ret_send,
                                ret_recv,
                                (peer, tp),
                            ).start()

                        return 0

                    lax.fori_loop(0, quarter, send, 0)

    advance(1)
    advance(2)
    with jax.named_scope("attention"):
        attention()
    mix_pair().start()
    for i in range(3):
        loads[i].wait()
        pair_copies[i].wait_recv()

    def one_step(step, _):
        every = all_but_one(
            arrived.at[lax.rem(step, NZ)], disp_send.at[0], disp_recv.at[lax.rem(step, NZ)]
        )
        with jax.named_scope("wait_arrived"):
            every.wait_recv()
        with jax.named_scope("experts"):
            experts(step)

        @pl.when(step + 2 <= NZ)
        def _():
            advance(step + 2)

        combine(step)

        @pl.when(step == 1)
        def _():
            with jax.named_scope("mixer"):
                mix_terms()

        return 0

    lax.fori_loop(1, NZ + 1, one_step, 0)
    returned[ep] = ring_out[NZ, position_here]

    peers = mix_in.at[pl.ds(1, NZ - 1)]
    remote(peers, peers, mix_send, mix_recv, sibling).wait()
    total = mix_out[z].astype(F32)
    for j in range(1, NZ):
        total = total + mix_in[j].astype(F32)
    attn_out[...] = total.astype(BF16)

    def column(row):
        return jnp.transpose(jnp.broadcast_to(row, (tokens, tokens)))[:, 0:1]

    slot_lane = iota((tokens, EP * CAP), 1).astype(F32)
    select_a = jnp.where(slot_lane == column(slots[0, 0][0:1]), 1.0, 0.0).astype(BF16)
    select_b = jnp.where(slot_lane == column(slots[0, 1][0:1]), 1.0, 0.0).astype(BF16)
    score_a, score_b = scores_ref[0:1, :], scores_ref[1:2, :]
    weight_a = column(1.0 / (1.0 + jnp.exp(score_b - score_a)))
    weight_b = column(1.0 / (jnp.exp(score_a - score_b) + 1.0))
    with jax.named_scope("wait_returned"):
        all_but_one(returned, ret_send, ret_recv).wait()
    results = returned[...].reshape(EP * CAP, width)
    result_a = jnp.dot(select_a, results, preferred_element_type=F32)
    result_b = jnp.dot(select_b, results, preferred_element_type=F32)
    expert_out[...] = (weight_a * result_a + weight_b * result_b).astype(BF16)

    for hop in range(1, 4):
        for chunk in range(2):
            ag_up(hop, chunk).wait_send()
            ag_down(hop, chunk).wait_send()
    ag_up(4, 0).wait_send()
    ag_down(4, 1).wait_send()
    mix_pair().wait_send()
    for copy in pair_copies:
        copy.wait_send()

    def drain_slots(j, _):
        slot_copy(j).wait_send()
        return 0

    lax.fori_loop(1, NZ, drain_slots, 0)

    def drain_kv(j, _):
        kv_copy(ep, j).wait_send()
        return 0

    lax.fori_loop(ep + 1, EP, drain_kv, 0)

    def drain_dispatch(step, _):
        all_but_one(outgoing.at[step], disp_send.at[step], disp_recv.at[step]).wait_send()
        return 0

    lax.fori_loop(0, NZ, drain_dispatch, 0)

    def drain_ring(step, _):
        for chunk in range(2):
            for part in range(2):
                ring(step, part, chunk).wait_send()
        return 0

    lax.fori_loop(1, NZ, drain_ring, 0)


def body(
    query_rows,
    key_rows,
    value_rows,
    query_norm_gain,
    key_gain,
    break_offset,
    mixer_out_weight,
    routed_tokens,
    expert_gain,
    routes,
    route_scores,
    gate_weight,
    up_weight,
    down_weight,
):
    rows = query_rows.shape[0]
    tokens, width = routed_tokens.shape
    units = gate_weight.shape[2]
    vmem = pl.BlockSpec(memory_space=pltpu.VMEM)
    smem = pl.BlockSpec(memory_space=pltpu.SMEM)
    hbm = pl.BlockSpec(memory_space=pl.ANY)
    dma = pltpu.SemaphoreType.DMA
    return pl.pallas_call(
        kernel,
        out_shape=(
            jax.ShapeDtypeStruct((rows // (2 * NZ), width), BF16),
            jax.ShapeDtypeStruct((tokens, width), BF16),
        ),
        in_specs=[vmem] * 5 + [smem, hbm] + [vmem] * 4 + [hbm] * 3,
        out_specs=(vmem, vmem),
        scratch_shapes=[
            pltpu.VMEM((2, units, width), BF16),
            pltpu.VMEM((2, units, width), BF16),
            pltpu.VMEM((2, units, width), BF16),
            pltpu.VMEM((2, 128, width), BF16),
            pltpu.VMEM((EP, 2, rows, 128), BF16),
            pltpu.VMEM((NZ, tokens, width), BF16),
            pltpu.VMEM((NZ, 2, 8, 128), F32),
            pltpu.VMEM((NZ, EP, CAP, width), BF16),
            pltpu.VMEM((NZ, EP, CAP, width), BF16),
            pltpu.VMEM((EP * CAP, width), F32),
            pltpu.VMEM((NZ + 1, EP, CAP, width), BF16),
            pltpu.VMEM((NZ + 1, EP, CAP, width), BF16),
            pltpu.VMEM((EP, CAP, width), BF16),
            pltpu.VMEM((2, 64, 128), BF16),
            pltpu.VMEM((64, 128), BF16),
            pltpu.VMEM((NZ, 8, width), BF16),
            pltpu.VMEM((NZ, 8, width), BF16),
            dma((4,)),
            dma((5,)),
            dma((5,)),
            dma((EP,)),
            dma((EP,)),
            dma((2, 5)),
            dma((2, 5)),
            dma((2, 5)),
            dma((2, 5)),
            dma((NZ,)),
            dma((NZ,)),
            dma((NZ,)),
            dma((NZ,)),
            dma((4, NZ + 1)),
            dma((4, NZ + 1)),
            dma,
            dma,
            dma,
            dma,
        ],
        compiler_params=pltpu.CompilerParams(
            collective_id=0, has_side_effects=True, vmem_limit_bytes=67043328
        ),
    )(
        query_rows,
        key_rows,
        value_rows,
        query_norm_gain[None, :],
        key_gain[None, :],
        break_offset,
        mixer_out_weight,
        routed_tokens,
        expert_gain[None, :],
        routes.T,
        route_scores.T,
        gate_weight[0].T,
        up_weight[0].T,
        down_weight[0],
    )


def solution(mesh):
    in_specs = (
        P("ep", "tp"),
        P("ep", "tp"),
        P("ep", "tp"),
        P(),
        P(),
        P("tp"),
        P("tp", None),
        P(("ep", "tp"), None),
        P(),
        P(("ep", "tp"), None),
        P(("ep", "tp"), None),
        P("ep", None, "tp"),
        P("ep", None, "tp"),
        P("ep", "tp", None),
    )
    out_specs = (P(("ep", "tp"), None), P(("ep", "tp"), None))
    return jax.shard_map(body, mesh=mesh, in_specs=in_specs, out_specs=out_specs, check_vma=False)
```

```python
import functools

import jax
import jax.numpy as jnp
from jax import lax
from jax.experimental import pallas as pl
from jax.experimental.pallas import tpu as pltpu
from jax.sharding import PartitionSpec as P

HEAD_DIM = 64
EPS = 1e-06
MESH = pl.DeviceIdType.MESH
EP = 16
NZ = 8
CAP = 16
HALF = EP // 2
PIECES = 2
CHUNKS = 4
F32 = jnp.float32
BF16 = jnp.bfloat16


def iota(shape, dim):
    return lax.broadcasted_iota(jnp.int32, shape, dim)


def kernel(
    query_hbm,
    key_hbm,
    value_hbm,
    query_gain_hbm,
    key_gain_hbm,
    offset_hbm,
    mixer_hbm,
    tokens_hbm,
    expert_gain_hbm,
    routes_hbm,
    scores_hbm,
    gate_hbm,
    up_hbm,
    down_hbm,
    attn_hbm,
    blend_hbm,
    returned,
    query_ref,
    key_ref,
    value_ref,
    query_gain_ref,
    key_gain_ref,
    offset_ref,
    tokens_ref,
    expert_gain_ref,
    routes_ref,
    scores_ref,
    gate_w,
    up_w,
    down_w,
    mixer_w,
    kv,
    tok,
    slots,
    outgoing,
    arrived,
    terms,
    ring_out,
    ring_in,
    blend,
    mix_mine,
    mix_theirs,
    mix_terms,
    mix_out,
    mix_in,
    load_sem,
    small_sem,
    pair_send,
    pair_recv,
    kv_send,
    kv_recv,
    up_send,
    up_recv,
    dn_send,
    dn_recv,
    slot_send,
    slot_recv,
    disp_send,
    disp_recv,
    ring_send,
    ring_recv,
    ret_send,
    ret_recv,
    mix_send,
    mix_recv,
):
    ep = lax.axis_index("ep")
    tp = lax.axis_index("tp")
    z, core = tp // 2, tp % 2
    above = (ep, lax.rem(z + 1, NZ) * 2 + core)
    below = (ep, lax.rem(z + NZ - 1, NZ) * 2 + core)
    sibling = (ep, z * 2 + 1 - core)
    rows = query_hbm.shape[0]
    tokens, width = tokens_hbm.shape
    position_here = lax.rem(ep // 4 + ep % 4, 4) * 4 + ep // 4
    goes_up = position_here < HALF

    def at_position(place):
        return place % 4 * 4 + lax.rem(place // 4 + 4 - place % 4, 4)

    def remote(src, dst, send, recv, device):
        return pltpu.make_async_remote_copy(
            src_ref=src,
            dst_ref=dst,
            send_sem=send,
            recv_sem=recv,
            device_id=device,
            device_id_type=MESH,
        )

    barrier = pltpu.get_barrier_semaphore()

    greeted = [(ep, lax.rem(z + j, NZ) * 2 + core) for j in range(1, NZ)]
    greeted += [(lax.rem(ep + j, EP), tp) for j in range(1, EP)] + [sibling]
    for peer in greeted:
        pl.semaphore_signal(barrier, inc=1, device_id=peer, device_id_type=MESH)

    operands = (
        (tokens_hbm, tokens_ref),
        (expert_gain_hbm, expert_gain_ref),
        (routes_hbm, routes_ref),
        (key_hbm, key_ref),
        (value_hbm, value_ref),
        (key_gain_hbm, key_gain_ref),
        (query_hbm, query_ref),
        (query_gain_hbm, query_gain_ref),
        (offset_hbm, offset_ref),
        (scores_hbm, scores_ref),
    )
    small = [
        pltpu.make_async_copy(src, dst, small_sem.at[i]) for i, (src, dst) in enumerate(operands)
    ]
    for copy in small:
        copy.start()

    weights = ((gate_hbm, gate_w), (up_hbm, up_w), (down_hbm, down_w), (mixer_hbm, mixer_w))
    loads = [
        pltpu.make_async_copy(src, dst.at[0], load_sem.at[i])
        for i, (src, dst) in enumerate(weights)
    ]
    for copy in loads:
        copy.start()

    lane = iota((rows, 128), 1)
    first_head = lane < HEAD_DIM

    def norm_heads(flat, gain):
        split = flat.astype(F32)
        squares = split * split
        mean_a = jnp.sum(jnp.where(first_head, squares, 0.0), axis=1, keepdims=True) / HEAD_DIM
        mean_b = jnp.sum(jnp.where(first_head, 0.0, squares), axis=1, keepdims=True) / HEAD_DIM
        scale = jnp.where(first_head, lax.rsqrt(mean_a + EPS), lax.rsqrt(mean_b + EPS))
        return (split * scale * jnp.concatenate([gain, gain], axis=1)).astype(BF16)

    for copy in small[:3]:
        copy.wait()
    as_float = tokens_ref[...].astype(F32)
    mean = jnp.mean(as_float * as_float, axis=1, keepdims=True)
    tok[0] = (as_float * lax.rsqrt(mean + EPS) * expert_gain_ref[...]).astype(BF16)

    expert_row = iota((EP, tokens), 0)
    member_a = jnp.where(routes_ref[0:1, :] == expert_row, 1.0, 0.0).astype(F32)
    member_b = jnp.where(routes_ref[1:2, :] == expert_row, 1.0, 0.0).astype(F32)
    earlier = jnp.where(iota((tokens, tokens), 0) < iota((tokens, tokens), 1), 1.0, 0.0)
    earlier = earlier.astype(BF16)
    ahead_a = jnp.dot(member_a.astype(BF16), earlier, preferred_element_type=F32)
    ahead_b = jnp.dot(member_b.astype(BF16), earlier, preferred_element_type=F32)
    ahead_b = ahead_b + jnp.sum(member_a, axis=1, keepdims=True)
    expert_base = (expert_row * CAP).astype(F32)
    slot_a = jnp.sum(member_a * (ahead_a + expert_base), axis=0, keepdims=True)
    slot_b = jnp.sum(member_b * (ahead_b + expert_base), axis=0, keepdims=True)
    slots[0, 0] = jnp.broadcast_to(slot_a, (8, tokens))
    slots[0, 1] = jnp.broadcast_to(slot_b, (8, tokens))

    for copy in small[3:]:
        copy.wait()
    key_norm = norm_heads(key_ref[...], key_gain_ref[...])
    kv[ep, 0] = key_norm
    kv[ep, 1] = value_ref[...]

    with jax.named_scope("wait_entry"):
        pl.semaphore_wait(barrier, len(greeted))

    part_tok = tokens // 2

    def ag_up(hop, chunk):
        part = pl.ds(chunk * part_tok, part_tok)
        return remote(
            tok.at[hop - 1, part],
            tok.at[hop, part],
            up_send.at[chunk, hop],
            up_recv.at[chunk, hop],
            above,
        )

    def ag_down(hop, chunk):
        part = pl.ds(chunk * part_tok, part_tok)
        return remote(
            tok.at[lax.rem(NZ + 1 - hop, NZ), part],
            tok.at[NZ - hop, part],
            dn_send.at[chunk, hop],
            dn_recv.at[chunk, hop],
            below,
        )

    def slot_copy(j):
        peer = (ep, lax.rem(z + j, NZ) * 2 + core)
        return remote(slots.at[0], slots.at[j], slot_send, slot_recv.at[j], peer)

    def send_slots(j, _):
        slot_copy(j).start()
        return 0

    lax.fori_loop(1, NZ, send_slots, 0)
    for chunk in range(2):
        ag_up(1, chunk).start()
        ag_down(1, 1 - chunk).start()

    def kv_copy(source, target):
        return remote(
            kv.at[source], kv.at[source], kv_send.at[target], kv_recv.at[source], (target, tp)
        )

    def send_kv(j, _):
        kv_copy(ep, j).start()
        return 0

    lax.fori_loop(ep + 1, EP, send_kv, 0)

    pair_copies = [
        remote(src, dst.at[1], pair_send.at[i], pair_recv.at[i], sibling)
        for i, (src, dst) in enumerate(weights)
    ]
    for copy in pair_copies:
        copy.start()

    slot_rows = iota((EP * CAP, tokens), 0).astype(F32)

    def dispatch(step, distance):
        row_a = slots[distance, 0][0:1]
        row_b = slots[distance, 1][0:1]
        pick = jnp.where((slot_rows == row_a) | (slot_rows == row_b), 1.0, 0.0).astype(BF16)
        picked = jnp.dot(pick, tok[distance], preferred_element_type=F32).astype(BF16)
        outgoing[pl.ds(step * EP, EP)] = picked.reshape(EP, CAP, width)

        def send(j, _):
            peer = lax.rem(ep + j, EP)
            remote(
                outgoing.at[step * EP + peer],
                arrived.at[step, position_here],
                disp_send,
                disp_recv.at[step],
                (peer, tp),
            ).start()
            return 0

        lax.fori_loop(1, EP, send, 0)
        arrived[step, position_here] = outgoing[step * EP + ep]

    def all_but_one(buffer, send, recv):
        block = buffer.at[pl.ds(0, EP - 1)]
        return remote(block, block, send, recv, sibling)

    def wait_slots(j, _):
        slot_copy(j).wait_recv()
        return 0

    def advance(step):
        @pl.when(step <= 3)
        def _():
            for chunk in range(2):
                with jax.named_scope("wait_up"):
                    ag_up(step, chunk).wait_recv()

                @pl.when(step <= 3 - chunk)
                def _():
                    ag_up(step + 1, chunk).start()

                with jax.named_scope("wait_down"):
                    ag_down(step, 1 - chunk).wait_recv()

                @pl.when(step <= 3 - chunk)
                def _():
                    ag_down(step + 1, 1 - chunk).start()

        @pl.when(step == 4)
        def _():
            with jax.named_scope("wait_last"):
                ag_up(4, 0).wait_recv()
                ag_down(4, 1).wait_recv()

        @pl.when(step == 1)
        def _():
            with jax.named_scope("wait_slots"):
                lax.fori_loop(1, NZ, wait_slots, 0)

        with jax.named_scope("dispatch"):
            distance = lax.rem(jnp.where(goes_up, step, NZ - step), NZ)
            dispatch(lax.rem(step, NZ), distance)

    def attention():
        query_norm = norm_heads(query_ref[...], query_gain_ref[...])
        zero = jnp.zeros_like(query_norm)
        queries = jnp.concatenate(
            [jnp.where(first_head, query_norm, zero), jnp.where(first_head, zero, query_norm)],
            axis=0,
        )
        row = iota((2 * rows, rows), 0)
        column = iota((2 * rows, rows), 1)
        offsets = jnp.where(row < rows, offset_ref[0], offset_ref[1])
        position = jnp.where(row < rows, row, row - rows)
        after = jnp.where(iota((rows, rows), 0) > iota((rows, rows), 1), 1.0, 0.0).astype(BF16)

        def absorb(j, state):
            mixed, carried = state

            @pl.when(j < ep)
            def _():
                kv_copy(j, ep).wait_recv()

            keys, values = kv[j, 0], kv[j, 1]
            scores = lax.dot_general(
                queries, keys, (((1,), (1,)), ((), ())), preferred_element_type=F32
            )
            scores = scores * HEAD_DIM ** (-0.5) + offsets
            allowed = (column < position) | (j < ep)
            log_fail = -(jnp.maximum(scores, 0.0) + jnp.log1p(jnp.exp(-jnp.abs(scores))))
            log_rise = scores + log_fail
            log_fail = jnp.where(allowed, log_fail, 0.0)
            high = log_fail.astype(BF16)
            rest = log_fail - high.astype(F32)
            middle = rest.astype(BF16)
            low = (rest - middle.astype(F32)).astype(BF16)
            between = (
                jnp.dot(high, after, preferred_element_type=F32)
                + jnp.dot(middle, after, preferred_element_type=F32)
                + jnp.dot(low, after, preferred_element_type=F32)
            )
            weights = jnp.where(allowed, jnp.exp(log_rise + between + carried), 0.0).astype(BF16)
            mixed = mixed + jnp.dot(weights, values, preferred_element_type=F32)
            carried = carried + jnp.sum(log_fail, axis=1, keepdims=True)
            return mixed, carried

        state = (jnp.zeros((2 * rows, 128), F32), jnp.zeros((2 * rows, 1), F32))
        mixed, _ = lax.fori_loop(0, ep + 1, lambda t, s: absorb(ep - t, s), state)
        heads = jnp.where(first_head, mixed[:rows], mixed[rows:]).astype(BF16)
        to_row = iota((rows, rows), 0)
        from_row = iota((rows, rows), 1)
        owner_core = to_row // 64
        within = to_row % 64
        source = (within // 8) * 16 + owner_core * 8 + within % 8
        order = jnp.where(from_row == source, 1.0, 0.0).astype(BF16)
        ordered = jnp.dot(order, heads, preferred_element_type=F32).astype(BF16)
        mix_mine[0] = ordered[:64]
        mix_mine[1] = ordered[64:]

    def mix_pair():
        return remote(
            mix_mine.at[1 - core], mix_theirs, pair_send.at[4], pair_recv.at[4], sibling
        )

    def project():
        loads[3].wait()
        pair_copies[3].wait_recv()
        mix_pair().wait_recv()
        term = jnp.dot(mix_mine[core], mixer_w[0], preferred_element_type=F32)
        term = term + jnp.dot(mix_theirs[...], mixer_w[1], preferred_element_type=F32)
        for i in range(NZ):
            for part in range(2):
                columns = slice(part * width // 2, (part + 1) * width // 2)
                mix_terms[i, part] = term[8 * i : 8 * i + 8, columns]

    def mix_ring(step, part):
        return remote(
            mix_out.at[step, part],
            mix_in.at[step + 1, part],
            mix_send,
            mix_recv.at[part, step + 1],
            (above, below)[part],
        )

    def mix(step):
        for part, owner in ((0, z + NZ - step), (1, z + step)):
            mine = mix_terms[lax.rem(owner, NZ), part]

            @pl.when(step == 1)
            def _():
                mix_out[step, part] = mine.astype(BF16)

            @pl.when(step >= 2)
            def _():
                with jax.named_scope("wait_mix"):
                    mix_ring(step - 1, part).wait_recv()
                mix_out[step, part] = (mine + mix_in[step, part].astype(F32)).astype(BF16)

            @pl.when(step < NZ)
            def _():
                mix_ring(step, part).start()

    def experts(step):
        rows_in = arrived[lax.rem(step, NZ)].reshape(EP * CAP, width)
        across = (((1,), (1,)), ((), ()))
        units = 2 * gate_w.shape[1]
        gate = lax.dot_general(
            rows_in, gate_w[...].reshape(units, width), across, preferred_element_type=F32
        )
        up = lax.dot_general(
            rows_in, up_w[...].reshape(units, width), across, preferred_element_type=F32
        )
        hidden = (gate / (1.0 + jnp.exp(-gate)) * up).astype(BF16)
        terms[...] = jnp.dot(
            hidden, down_w[...].reshape(units, width), preferred_element_type=F32
        )

    share = EP // (2 * CHUNKS)
    share_rows = share * CAP

    def ring(step, part, chunk):
        blocks = pl.ds((part * CHUNKS + chunk) * share, share)
        return remote(
            ring_out.at[step, blocks],
            ring_in.at[step + 1, blocks],
            ring_send,
            ring_recv.at[part * CHUNKS + chunk, step + 1],
            (above, below)[part],
        )

    def combine(step):
        for chunk in range(CHUNKS):
            for part in range(2):
                first = (part * CHUNKS + chunk) * share
                blocks = pl.ds(first, share)
                mine = terms[first * CAP : (first + share) * CAP, :]

                @pl.when(step == 1)
                def _():
                    ring_out[step, blocks] = mine.astype(BF16).reshape(share, CAP, width)

                @pl.when(step >= 2)
                def _():
                    with jax.named_scope("wait_ring"):
                        ring(step - 1, part, chunk).wait_recv()
                    sofar = ring_in[step, blocks].reshape(share_rows, width).astype(F32)
                    total = (mine + sofar).astype(BF16)
                    ring_out[step, blocks] = total.reshape(share, CAP, width)

                @pl.when(step < NZ)
                def _():
                    ring(step, part, chunk).start()

                @pl.when(step == NZ)
                def _():
                    def send(j, _):
                        peer = at_position(first + j)

                        @pl.when(peer != ep)
                        def _():
                            remote(
                                ring_out.at[NZ, first + j],
                                returned.at[ep],
                                ret_send,
                                ret_recv,
                                (peer, tp),
                            ).start()

                        return 0

                    lax.fori_loop(0, share, send, 0)

    advance(1)
    advance(2)
    with jax.named_scope("attention"):
        attention()
    mix_pair().start()
    for i in range(3):
        loads[i].wait()
        pair_copies[i].wait_recv()

    def one_step(step, _):
        every = all_but_one(
            arrived.at[lax.rem(step, NZ)], disp_send, disp_recv.at[lax.rem(step, NZ)]
        )
        with jax.named_scope("wait_arrived"):
            every.wait_recv()
        with jax.named_scope("experts"):
            experts(step)

        @pl.when(step <= 2)
        def _():
            advance(step + 2)

        combine(step)

        @pl.when((step >= 2) & (step + 3 <= NZ))
        def _():
            advance(step + 3)

        @pl.when(step == 1)
        def _():
            with jax.named_scope("mixer"):
                project()

        mix(step)

        return 0

    lax.fori_loop(1, NZ + 1, one_step, 0)
    own = pltpu.make_async_copy(ring_out.at[NZ, position_here], returned.at[ep], load_sem.at[4])
    own.start()
    attn_copy = pltpu.make_async_copy(mix_out.at[NZ], attn_hbm, load_sem.at[6])
    attn_copy.start()

    def column(row):
        return jnp.transpose(jnp.broadcast_to(row, (tokens, tokens)))[:, 0:1]

    slot_lane = iota((tokens, EP * CAP), 1).astype(F32)
    score_a, score_b = scores_ref[0:1, :], scores_ref[1:2, :]
    weight_a = column(1.0 / (1.0 + jnp.exp(score_b - score_a)))
    weight_b = column(1.0 / (jnp.exp(score_a - score_b) + 1.0))
    weight = jnp.where(slot_lane == column(slots[0, 0][0:1]), weight_a, 0.0)
    weight = jnp.where(slot_lane == column(slots[0, 1][0:1]), weight_b, weight)
    high = weight.astype(BF16)
    blend[0] = high
    blend[1] = (weight - high.astype(F32)).astype(BF16)
    blend_copy = pltpu.make_async_copy(blend, blend_hbm, load_sem.at[5])
    blend_copy.start()

    for hop in range(1, 4):
        for chunk in range(2):
            ag_up(hop, chunk).wait_send()
            ag_down(hop, chunk).wait_send()
    ag_up(4, 0).wait_send()
    ag_down(4, 1).wait_send()
    mix_pair().wait_send()
    for copy in pair_copies:
        copy.wait_send()

    def drain(block, send, recv):
        remote(block, block, send, recv, sibling).wait_send()

    drain(slots.at[pl.ds(1, NZ - 1)], slot_send, slot_recv.at[0])
    drain(outgoing.at[pl.ds(0, NZ * (EP - 1))], disp_send, disp_recv.at[0])
    drain(mix_out.at[pl.ds(1, NZ - 1)], mix_send, mix_recv.at[0, 0])
    drain(ring_out.at[pl.ds(1, NZ - 1)], ring_send, ring_recv.at[0, 0])

    def drain_kv(j, _):
        kv_copy(ep, j).wait_send()
        return 0

    lax.fori_loop(ep + 1, EP, drain_kv, 0)

    with jax.named_scope("wait_returned"):
        own.wait()
        blend_copy.wait()
        all_but_one(returned, ret_send, ret_recv).wait()
        attn_copy.wait()


def blend_kernel(blend_ref, results_ref, attn_ref, expert_out, attn_out):
    _, tokens, slots = blend_ref.shape
    parts = jnp.dot(
        blend_ref[...].reshape(2 * tokens, slots), results_ref[...], preferred_element_type=F32
    )
    expert_out[...] = (parts[:tokens] + parts[tokens:]).astype(BF16)

    @pl.when(pl.program_id(0) == 0)
    def _():
        half = attn_ref.shape[2]
        attn_out[:, :half] = attn_ref[0]
        attn_out[:, half:] = attn_ref[1]


def body(
    query_rows,
    key_rows,
    value_rows,
    query_norm_gain,
    key_gain,
    break_offset,
    mixer_out_weight,
    routed_tokens,
    expert_gain,
    routes,
    route_scores,
    gate_weight,
    up_weight,
    down_weight,
):
    rows = query_rows.shape[0]
    tokens, width = routed_tokens.shape
    units = gate_weight.shape[2]
    hbm = pl.BlockSpec(memory_space=pl.ANY)
    dma = pltpu.SemaphoreType.DMA
    attn, blend, returned = pl.pallas_call(
        kernel,
        out_shape=(
            jax.ShapeDtypeStruct((2, rows // (2 * NZ), width // 2), BF16),
            jax.ShapeDtypeStruct((2, tokens, EP * CAP), BF16),
            jax.ShapeDtypeStruct((EP, CAP, width), BF16),
        ),
        in_specs=[hbm] * 14,
        out_specs=(hbm, hbm, hbm),
        scratch_shapes=[
            pltpu.VMEM((rows, 128), BF16),
            pltpu.VMEM((rows, 128), BF16),
            pltpu.VMEM((rows, 128), BF16),
            pltpu.VMEM((1, HEAD_DIM), F32),
            pltpu.VMEM((1, HEAD_DIM), F32),
            pltpu.SMEM((2,), F32),
            pltpu.VMEM((tokens, width), BF16),
            pltpu.VMEM((1, width), F32),
            pltpu.VMEM((2, tokens), jnp.int32),
            pltpu.VMEM((2, tokens), F32),
            pltpu.VMEM((2, units, width), BF16),
            pltpu.VMEM((2, units, width), BF16),
            pltpu.VMEM((2, units, width), BF16),
            pltpu.VMEM((2, 128, width), BF16),
            pltpu.VMEM((EP, 2, rows, 128), BF16),
            pltpu.VMEM((NZ, tokens, width), BF16),
            pltpu.VMEM((NZ, 2, 8, 128), F32),
            pltpu.VMEM((NZ * EP, CAP, width), BF16),
            pltpu.VMEM((NZ, EP, CAP, width), BF16),
            pltpu.VMEM((EP * CAP, width), F32),
            pltpu.VMEM((NZ + 1, EP, CAP, width), BF16),
            pltpu.VMEM((NZ + 1, EP, CAP, width), BF16),
            pltpu.VMEM((2, tokens, EP * CAP), BF16),
            pltpu.VMEM((2, 64, 128), BF16),
            pltpu.VMEM((64, 128), BF16),
            pltpu.VMEM((NZ, 2, 8, width // 2), F32),
            pltpu.VMEM((NZ + 1, 2, 8, width // 2), BF16),
            pltpu.VMEM((NZ + 1, 2, 8, width // 2), BF16),
            dma((7,)),
            dma((10,)),
            dma((5,)),
            dma((5,)),
            dma((EP,)),
            dma((EP,)),
            dma((2, 5)),
            dma((2, 5)),
            dma((2, 5)),
            dma((2, 5)),
            dma,
            dma((NZ,)),
            dma,
            dma((NZ,)),
            dma,
            dma((2 * CHUNKS, NZ + 1)),
            dma,
            dma,
            dma,
            dma((2, NZ + 1)),
        ],
        compiler_params=pltpu.CompilerParams(
            collective_id=0, has_side_effects=True, vmem_limit_bytes=67043328
        ),
    )(
        query_rows,
        key_rows,
        value_rows,
        query_norm_gain[None, :],
        key_gain[None, :],
        break_offset,
        mixer_out_weight,
        routed_tokens,
        expert_gain[None, :],
        routes.T,
        route_scores.T,
        gate_weight[0].T,
        up_weight[0].T,
        down_weight[0],
    )
    piece = width // PIECES
    expert_output, attention_output = pl.pallas_call(
        blend_kernel,
        grid=(PIECES,),
        out_shape=(
            jax.ShapeDtypeStruct((tokens, width), BF16),
            jax.ShapeDtypeStruct((rows // (2 * NZ), width), BF16),
        ),
        in_specs=[
            pl.BlockSpec(blend.shape, lambda i: (0, 0, 0)),
            pl.BlockSpec((EP * CAP, piece), lambda i: (0, i)),
            pl.BlockSpec(attn.shape, lambda i: (0, 0, 0)),
        ],
        out_specs=(
            pl.BlockSpec((tokens, piece), lambda i: (0, i)),
            pl.BlockSpec((rows // (2 * NZ), width), lambda i: (0, 0)),
        ),
    )(blend, returned.reshape(EP * CAP, width), attn)
    return attention_output, expert_output


def solution(mesh):
    in_specs = (
        P("ep", "tp"),
        P("ep", "tp"),
        P("ep", "tp"),
        P(),
        P(),
        P("tp"),
        P("tp", None),
        P(("ep", "tp"), None),
        P(),
        P(("ep", "tp"), None),
        P(("ep", "tp"), None),
        P("ep", None, "tp"),
        P("ep", None, "tp"),
        P("ep", "tp", None),
    )
    out_specs = (P(("ep", "tp"), None), P(("ep", "tp"), None))
    return jax.shard_map(body, mesh=mesh, in_specs=in_specs, out_specs=out_specs, check_vma=False)
```

```python
import functools

import jax
import jax.numpy as jnp
from jax import lax
from jax.experimental import pallas as pl
from jax.experimental.pallas import tpu as pltpu
from jax.sharding import PartitionSpec as P

HEAD_DIM = 64
EPS = 1e-06
MESH = pl.DeviceIdType.MESH
EP = 16
NZ = 8
CAP = 16
HALF = EP // 2
PIECES = 2
CHUNKS = 4
F32 = jnp.float32
BF16 = jnp.bfloat16


def iota(shape, dim):
    return lax.broadcasted_iota(jnp.int32, shape, dim)


def kernel(
    query_hbm,
    key_hbm,
    value_hbm,
    query_gain_hbm,
    key_gain_hbm,
    offset_hbm,
    mixer_hbm,
    tokens_hbm,
    expert_gain_hbm,
    routes_hbm,
    scores_hbm,
    gate_hbm,
    up_hbm,
    down_hbm,
    attn_hbm,
    blend_hbm,
    returned,
    query_ref,
    key_ref,
    value_ref,
    query_gain_ref,
    key_gain_ref,
    offset_ref,
    tokens_ref,
    expert_gain_ref,
    routes_ref,
    scores_ref,
    gate_w,
    up_w,
    down_w,
    mixer_w,
    kv,
    tok,
    slots,
    outgoing,
    arrived,
    terms,
    ring_out,
    ring_in,
    blend,
    mix_mine,
    mix_theirs,
    mix_terms,
    mix_out,
    mix_in,
    load_sem,
    small_sem,
    pair_send,
    pair_recv,
    kv_send,
    kv_recv,
    ag_send,
    up_recv,
    dn_recv,
    slot_send,
    slot_recv,
    disp_send,
    disp_recv,
    ring_send,
    ring_recv,
    ret_send,
    ret_recv,
    mix_send,
    mix_recv,
):
    ep = lax.axis_index("ep")
    tp = lax.axis_index("tp")
    z, core = tp // 2, tp % 2
    above = (ep, lax.rem(z + 1, NZ) * 2 + core)
    below = (ep, lax.rem(z + NZ - 1, NZ) * 2 + core)
    sibling = (ep, z * 2 + 1 - core)
    rows = query_hbm.shape[0]
    tokens, width = tokens_hbm.shape
    position_here = lax.rem(ep // 4 + ep % 4, 4) * 4 + ep // 4
    goes_up = position_here < HALF

    def at_position(place):
        return place % 4 * 4 + lax.rem(place // 4 + 4 - place % 4, 4)

    def remote(src, dst, send, recv, device):
        return pltpu.make_async_remote_copy(
            src_ref=src,
            dst_ref=dst,
            send_sem=send,
            recv_sem=recv,
            device_id=device,
            device_id_type=MESH,
        )

    barrier = pltpu.get_barrier_semaphore()

    greeted = [(ep, lax.rem(z + j, NZ) * 2 + core) for j in range(1, NZ)]
    greeted += [(lax.rem(ep + j, EP), tp) for j in range(1, EP)] + [sibling]
    for peer in greeted:
        pl.semaphore_signal(barrier, inc=1, device_id=peer, device_id_type=MESH)

    operands = (
        (tokens_hbm, tokens_ref),
        (expert_gain_hbm, expert_gain_ref),
        (routes_hbm, routes_ref),
        (key_hbm, key_ref),
        (value_hbm, value_ref),
        (key_gain_hbm, key_gain_ref),
        (query_hbm, query_ref),
        (query_gain_hbm, query_gain_ref),
        (offset_hbm, offset_ref),
        (scores_hbm, scores_ref),
    )
    small = [
        pltpu.make_async_copy(src, dst, small_sem.at[i]) for i, (src, dst) in enumerate(operands)
    ]
    for copy in small:
        copy.start()

    weights = ((gate_hbm, gate_w), (up_hbm, up_w), (down_hbm, down_w), (mixer_hbm, mixer_w))
    loads = [
        pltpu.make_async_copy(src, dst.at[0], load_sem.at[i])
        for i, (src, dst) in enumerate(weights)
    ]
    for copy in loads:
        copy.start()

    lane = iota((rows, 128), 1)
    first_head = lane < HEAD_DIM

    def norm_heads(flat, gain):
        split = flat.astype(F32)
        squares = split * split
        mean_a = jnp.sum(jnp.where(first_head, squares, 0.0), axis=1, keepdims=True) / HEAD_DIM
        mean_b = jnp.sum(jnp.where(first_head, 0.0, squares), axis=1, keepdims=True) / HEAD_DIM
        scale = jnp.where(first_head, lax.rsqrt(mean_a + EPS), lax.rsqrt(mean_b + EPS))
        return (split * scale * jnp.concatenate([gain, gain], axis=1)).astype(BF16)

    for copy in small[:3]:
        copy.wait()
    as_float = tokens_ref[...].astype(F32)
    mean = jnp.mean(as_float * as_float, axis=1, keepdims=True)
    tok[0] = (as_float * lax.rsqrt(mean + EPS) * expert_gain_ref[...]).astype(BF16)

    expert_row = iota((EP, tokens), 0)
    member_a = jnp.where(routes_ref[0:1, :] == expert_row, 1.0, 0.0).astype(F32)
    member_b = jnp.where(routes_ref[1:2, :] == expert_row, 1.0, 0.0).astype(F32)
    earlier = jnp.where(iota((tokens, tokens), 0) < iota((tokens, tokens), 1), 1.0, 0.0)
    earlier = earlier.astype(BF16)
    ahead_a = jnp.dot(member_a.astype(BF16), earlier, preferred_element_type=F32)
    ahead_b = jnp.dot(member_b.astype(BF16), earlier, preferred_element_type=F32)
    ahead_b = ahead_b + jnp.sum(member_a, axis=1, keepdims=True)
    expert_base = (expert_row * CAP).astype(F32)
    slot_a = jnp.sum(member_a * (ahead_a + expert_base), axis=0, keepdims=True)
    slot_b = jnp.sum(member_b * (ahead_b + expert_base), axis=0, keepdims=True)
    slots[0, 0] = jnp.broadcast_to(slot_a, (8, tokens))
    slots[0, 1] = jnp.broadcast_to(slot_b, (8, tokens))

    with jax.named_scope("wait_entry"):
        pl.semaphore_wait(barrier, len(greeted))

    part_tok = tokens // 2

    def ag_up(hop, chunk):
        part = pl.ds(chunk * part_tok, part_tok)
        return remote(
            tok.at[hop - 1, part],
            tok.at[hop, part],
            ag_send,
            up_recv.at[chunk, hop],
            above,
        )

    def ag_down(hop, chunk):
        part = pl.ds(chunk * part_tok, part_tok)
        return remote(
            tok.at[lax.rem(NZ + 1 - hop, NZ), part],
            tok.at[NZ - hop, part],
            ag_send,
            dn_recv.at[chunk, hop],
            below,
        )

    def slot_copy(j):
        peer = (ep, lax.rem(z + j, NZ) * 2 + core)
        return remote(slots.at[0], slots.at[j], slot_send, slot_recv.at[j], peer)

    def send_slots(j, _):
        slot_copy(j).start()
        return 0

    lax.fori_loop(1, NZ, send_slots, 0)
    for chunk in range(2):
        ag_up(1, chunk).start()
        ag_down(1, 1 - chunk).start()

    for copy in small[3:]:
        copy.wait()
    key_norm = norm_heads(key_ref[...], key_gain_ref[...])
    kv[ep, 0] = key_norm
    kv[ep, 1] = value_ref[...]

    def kv_copy(source, target):
        return remote(
            kv.at[source], kv.at[source], kv_send.at[target], kv_recv.at[source], (target, tp)
        )

    def send_kv(j, _):
        kv_copy(ep, j).start()
        return 0

    lax.fori_loop(ep + 1, EP, send_kv, 0)

    pair_copies = [
        remote(src, dst.at[1], pair_send.at[i], pair_recv.at[i], sibling)
        for i, (src, dst) in enumerate(weights)
    ]
    for copy in pair_copies:
        copy.start()

    slot_rows = iota((EP * CAP, tokens), 0).astype(F32)

    def dispatch(step, distance):
        row_a = slots[distance, 0][0:1]
        row_b = slots[distance, 1][0:1]
        pick = jnp.where((slot_rows == row_a) | (slot_rows == row_b), 1.0, 0.0).astype(BF16)
        picked = jnp.dot(pick, tok[distance], preferred_element_type=F32).astype(BF16)
        outgoing[pl.ds(step * EP, EP)] = picked.reshape(EP, CAP, width)

        def send(j, _):
            peer = lax.rem(ep + j, EP)
            remote(
                outgoing.at[step * EP + peer],
                arrived.at[step, position_here],
                disp_send,
                disp_recv.at[step],
                (peer, tp),
            ).start()
            return 0

        lax.fori_loop(1, EP, send, 0)
        arrived[step, position_here] = outgoing[step * EP + ep]

    def all_but_one(buffer, send, recv):
        block = buffer.at[pl.ds(0, EP - 1)]
        return remote(block, block, send, recv, sibling)

    def wait_slots(j, _):
        slot_copy(j).wait_recv()
        return 0

    def advance(step):
        @pl.when(step <= 3)
        def _():
            for chunk in range(2):
                with jax.named_scope("wait_up"):
                    ag_up(step, chunk).wait_recv()

                @pl.when(step <= 3 - chunk)
                def _():
                    ag_up(step + 1, chunk).start()

                with jax.named_scope("wait_down"):
                    ag_down(step, 1 - chunk).wait_recv()

                @pl.when(step <= 3 - chunk)
                def _():
                    ag_down(step + 1, 1 - chunk).start()

        @pl.when(step == 4)
        def _():
            with jax.named_scope("wait_last"):
                ag_up(4, 0).wait_recv()
                ag_down(4, 1).wait_recv()

        @pl.when(step == 1)
        def _():
            with jax.named_scope("wait_slots"):
                lax.fori_loop(1, NZ, wait_slots, 0)

        with jax.named_scope("dispatch"):
            distance = lax.rem(jnp.where(goes_up, step, NZ - step), NZ)
            dispatch(lax.rem(step, NZ), distance)

    def attention():
        query_norm = norm_heads(query_ref[...], query_gain_ref[...])
        zero = jnp.zeros_like(query_norm)
        queries = jnp.concatenate(
            [jnp.where(first_head, query_norm, zero), jnp.where(first_head, zero, query_norm)],
            axis=0,
        )
        row = iota((2 * rows, rows), 0)
        column = iota((2 * rows, rows), 1)
        offsets = jnp.where(row < rows, offset_ref[0], offset_ref[1])
        position = jnp.where(row < rows, row, row - rows)
        after = jnp.where(iota((rows, rows), 0) > iota((rows, rows), 1), 1.0, 0.0).astype(BF16)

        def absorb(j, state):
            mixed, carried = state

            @pl.when(j < ep)
            def _():
                kv_copy(j, ep).wait_recv()

            keys, values = kv[j, 0], kv[j, 1]
            scores = lax.dot_general(
                queries, keys, (((1,), (1,)), ((), ())), preferred_element_type=F32
            )
            scores = scores * HEAD_DIM ** (-0.5) + offsets
            allowed = (column < position) | (j < ep)
            log_fail = -(jnp.maximum(scores, 0.0) + jnp.log1p(jnp.exp(-jnp.abs(scores))))
            log_rise = scores + log_fail
            log_fail = jnp.where(allowed, log_fail, 0.0)
            high = log_fail.astype(BF16)
            rest = log_fail - high.astype(F32)
            middle = rest.astype(BF16)
            low = (rest - middle.astype(F32)).astype(BF16)
            between = (
                jnp.dot(high, after, preferred_element_type=F32)
                + jnp.dot(middle, after, preferred_element_type=F32)
                + jnp.dot(low, after, preferred_element_type=F32)
            )
            weights = jnp.where(allowed, jnp.exp(log_rise + between + carried), 0.0).astype(BF16)
            mixed = mixed + jnp.dot(weights, values, preferred_element_type=F32)
            carried = carried + jnp.sum(log_fail, axis=1, keepdims=True)
            return mixed, carried

        state = (jnp.zeros((2 * rows, 128), F32), jnp.zeros((2 * rows, 1), F32))
        mixed, _ = lax.fori_loop(0, ep + 1, lambda t, s: absorb(ep - t, s), state)
        heads = jnp.where(first_head, mixed[:rows], mixed[rows:]).astype(BF16)
        to_row = iota((rows, rows), 0)
        from_row = iota((rows, rows), 1)
        owner_core = to_row // 64
        within = to_row % 64
        source = (within // 8) * 16 + owner_core * 8 + within % 8
        order = jnp.where(from_row == source, 1.0, 0.0).astype(BF16)
        ordered = jnp.dot(order, heads, preferred_element_type=F32).astype(BF16)
        mix_mine[0] = ordered[:64]
        mix_mine[1] = ordered[64:]

    def mix_pair():
        return remote(
            mix_mine.at[1 - core], mix_theirs, pair_send.at[4], pair_recv.at[4], sibling
        )

    def project():
        loads[3].wait()
        pair_copies[3].wait_recv()
        mix_pair().wait_recv()
        term = jnp.dot(mix_mine[core], mixer_w[0], preferred_element_type=F32)
        term = term + jnp.dot(mix_theirs[...], mixer_w[1], preferred_element_type=F32)
        for i in range(NZ):
            for part in range(2):
                columns = slice(part * width // 2, (part + 1) * width // 2)
                mix_terms[i, part] = term[8 * i : 8 * i + 8, columns]

    def mix_ring(step, part):
        return remote(
            mix_out.at[step, part],
            mix_in.at[step + 1, part],
            mix_send,
            mix_recv.at[part, step + 1],
            (above, below)[part],
        )

    def mix(step):
        for part, owner in ((0, z + NZ - step), (1, z + step)):
            mine = mix_terms[lax.rem(owner, NZ), part]

            @pl.when(step == 1)
            def _():
                mix_out[step, part] = mine.astype(BF16)

            @pl.when(step >= 2)
            def _():
                with jax.named_scope("wait_mix"):
                    mix_ring(step - 1, part).wait_recv()
                mix_out[step, part] = (mine + mix_in[step, part].astype(F32)).astype(BF16)

            @pl.when(step < NZ)
            def _():
                mix_ring(step, part).start()

    def experts(step):
        rows_in = arrived[lax.rem(step, NZ)].reshape(EP * CAP, width)
        across = (((1,), (1,)), ((), ()))
        units = 2 * gate_w.shape[1]
        gate = lax.dot_general(
            rows_in, gate_w[...].reshape(units, width), across, preferred_element_type=F32
        )
        up = lax.dot_general(
            rows_in, up_w[...].reshape(units, width), across, preferred_element_type=F32
        )
        hidden = (gate / (1.0 + jnp.exp(-gate)) * up).astype(BF16)
        terms[...] = jnp.dot(
            hidden, down_w[...].reshape(units, width), preferred_element_type=F32
        )

    share = width // CHUNKS

    def ring(step, part, chunk):
        block = (pl.ds(part * HALF, HALF), slice(None), pl.ds(chunk * share, share))
        return remote(
            ring_out.at[step, *block],
            ring_in.at[step - 1, *block],
            ring_send,
            ring_recv.at[part * CHUNKS + chunk, step - 1],
            (above, below)[part],
        )

    def combine(step):
        for chunk in range(CHUNKS):
            columns = slice(chunk * share, (chunk + 1) * share)
            for part in range(2):
                blocks = pl.ds(part * HALF, HALF)
                mine = terms[part * HALF * CAP : (part + 1) * HALF * CAP, columns]

                @pl.when(step == 1)
                def _():
                    ring_out[step, blocks, :, columns] = mine.astype(BF16).reshape(HALF, CAP, share)

                @pl.when(step >= 2)
                def _():
                    with jax.named_scope("wait_ring"):
                        ring(step - 1, part, chunk).wait_recv()
                    sofar = ring_in[step - 2, blocks, :, columns].reshape(HALF * CAP, share)
                    total = (mine + sofar.astype(F32)).astype(BF16)
                    ring_out[step, blocks, :, columns] = total.reshape(HALF, CAP, share)

                @pl.when(step < NZ)
                def _():
                    ring(step, part, chunk).start()

                @pl.when(step == NZ)
                def _():
                    def send(j, _):
                        place = part * HALF + j
                        peer = at_position(place)

                        @pl.when(peer != ep)
                        def _():
                            remote(
                                ring_out.at[NZ, place, :, pl.ds(chunk * share, share)],
                                returned.at[ep, :, pl.ds(chunk * share, share)],
                                ret_send,
                                ret_recv,
                                (peer, tp),
                            ).start()

                        return 0

                    lax.fori_loop(0, HALF, send, 0)

    advance(1)
    advance(2)
    with jax.named_scope("attention"):
        attention()
    mix_pair().start()
    for i in range(3):
        loads[i].wait()
        pair_copies[i].wait_recv()

    def one_step(step, _):
        every = all_but_one(
            arrived.at[lax.rem(step, NZ)], disp_send, disp_recv.at[lax.rem(step, NZ)]
        )
        with jax.named_scope("wait_arrived"):
            every.wait_recv()
        with jax.named_scope("experts"):
            experts(step)

        @pl.when(step <= 2)
        def _():
            advance(step + 2)

        combine(step)

        @pl.when((step >= 2) & (step + 3 <= NZ))
        def _():
            advance(step + 3)

        @pl.when(step == 1)
        def _():
            with jax.named_scope("mixer"):
                project()

        mix(step)

        return 0

    lax.fori_loop(1, NZ + 1, one_step, 0)
    own = pltpu.make_async_copy(ring_out.at[NZ, position_here], returned.at[ep], load_sem.at[4])
    own.start()
    attn_copy = pltpu.make_async_copy(mix_out.at[NZ], attn_hbm, load_sem.at[6])
    attn_copy.start()

    def column(row):
        return jnp.transpose(jnp.broadcast_to(row, (tokens, tokens)))[:, 0:1]

    slot_lane = iota((tokens, EP * CAP), 1).astype(F32)
    score_a, score_b = scores_ref[0:1, :], scores_ref[1:2, :]
    weight_a = column(1.0 / (1.0 + jnp.exp(score_b - score_a)))
    weight_b = column(1.0 / (jnp.exp(score_a - score_b) + 1.0))
    weight = jnp.where(slot_lane == column(slots[0, 0][0:1]), weight_a, 0.0)
    weight = jnp.where(slot_lane == column(slots[0, 1][0:1]), weight_b, weight)
    high = weight.astype(BF16)
    blend[0] = high
    blend[1] = (weight - high.astype(F32)).astype(BF16)
    blend_copy = pltpu.make_async_copy(blend, blend_hbm, load_sem.at[5])
    blend_copy.start()

    mix_pair().wait_send()
    for copy in pair_copies:
        copy.wait_send()

    def drain(block, send, recv):
        remote(block, block, send, recv, sibling).wait_send()

    drain(tok.at[pl.ds(0, NZ - 1)], ag_send, up_recv.at[0, 0])
    drain(slots.at[pl.ds(1, NZ - 1)], slot_send, slot_recv.at[0])
    drain(outgoing.at[pl.ds(0, NZ * (EP - 1))], disp_send, disp_recv.at[0])
    drain(mix_out.at[pl.ds(1, NZ - 1)], mix_send, mix_recv.at[0, 0])
    drain(ring_out.at[pl.ds(1, NZ - 1)], ring_send, ring_recv.at[0, 0])

    def drain_kv(j, _):
        kv_copy(ep, j).wait_send()
        return 0

    lax.fori_loop(ep + 1, EP, drain_kv, 0)

    with jax.named_scope("wait_returned"):
        own.wait()
        blend_copy.wait()
        all_but_one(returned, ret_send, ret_recv).wait()
        attn_copy.wait()


def blend_kernel(blend_ref, results_ref, attn_ref, expert_out, attn_out):
    _, tokens, slots = blend_ref.shape
    parts = jnp.dot(
        blend_ref[...].reshape(2 * tokens, slots), results_ref[...], preferred_element_type=F32
    )
    expert_out[...] = (parts[:tokens] + parts[tokens:]).astype(BF16)

    @pl.when(pl.program_id(0) == 0)
    def _():
        half = attn_ref.shape[2]
        attn_out[:, :half] = attn_ref[0]
        attn_out[:, half:] = attn_ref[1]


def body(
    query_rows,
    key_rows,
    value_rows,
    query_norm_gain,
    key_gain,
    break_offset,
    mixer_out_weight,
    routed_tokens,
    expert_gain,
    routes,
    route_scores,
    gate_weight,
    up_weight,
    down_weight,
):
    rows = query_rows.shape[0]
    tokens, width = routed_tokens.shape
    units = gate_weight.shape[2]
    hbm = pl.BlockSpec(memory_space=pl.ANY)
    dma = pltpu.SemaphoreType.DMA
    attn, blend, returned = pl.pallas_call(
        kernel,
        out_shape=(
            jax.ShapeDtypeStruct((2, rows // (2 * NZ), width // 2), BF16),
            jax.ShapeDtypeStruct((2, tokens, EP * CAP), BF16),
            jax.ShapeDtypeStruct((EP, CAP, width), BF16),
        ),
        in_specs=[hbm] * 14,
        out_specs=(hbm, hbm, hbm),
        scratch_shapes=[
            pltpu.VMEM((rows, 128), BF16),
            pltpu.VMEM((rows, 128), BF16),
            pltpu.VMEM((rows, 128), BF16),
            pltpu.VMEM((1, HEAD_DIM), F32),
            pltpu.VMEM((1, HEAD_DIM), F32),
            pltpu.SMEM((2,), F32),
            pltpu.VMEM((tokens, width), BF16),
            pltpu.VMEM((1, width), F32),
            pltpu.VMEM((2, tokens), jnp.int32),
            pltpu.VMEM((2, tokens), F32),
            pltpu.VMEM((2, units, width), BF16),
            pltpu.VMEM((2, units, width), BF16),
            pltpu.VMEM((2, units, width), BF16),
            pltpu.VMEM((2, 128, width), BF16),
            pltpu.VMEM((EP, 2, rows, 128), BF16),
            pltpu.VMEM((NZ, tokens, width), BF16),
            pltpu.VMEM((NZ, 2, 8, 128), F32),
            pltpu.VMEM((NZ * EP, CAP, width), BF16),
            pltpu.VMEM((NZ, EP, CAP, width), BF16),
            pltpu.VMEM((EP * CAP, width), F32),
            pltpu.VMEM((NZ + 1, EP, CAP, width), BF16),
            pltpu.VMEM((NZ - 1, EP, CAP, width), BF16),
            pltpu.VMEM((2, tokens, EP * CAP), BF16),
            pltpu.VMEM((2, 64, 128), BF16),
            pltpu.VMEM((64, 128), BF16),
            pltpu.VMEM((NZ, 2, 8, width // 2), F32),
            pltpu.VMEM((NZ + 1, 2, 8, width // 2), BF16),
            pltpu.VMEM((NZ + 1, 2, 8, width // 2), BF16),
            dma((7,)),
            dma((10,)),
            dma((5,)),
            dma((5,)),
            dma((EP,)),
            dma((EP,)),
            dma,
            dma((2, 5)),
            dma((2, 5)),
            dma,
            dma((NZ,)),
            dma,
            dma((NZ,)),
            dma,
            dma((2 * CHUNKS, NZ - 1)),
            dma,
            dma,
            dma,
            dma((2, NZ + 1)),
        ],
        compiler_params=pltpu.CompilerParams(
            collective_id=0, has_side_effects=True, vmem_limit_bytes=67043328
        ),
    )(
        query_rows,
        key_rows,
        value_rows,
        query_norm_gain[None, :],
        key_gain[None, :],
        break_offset,
        mixer_out_weight,
        routed_tokens,
        expert_gain[None, :],
        routes.T,
        route_scores.T,
        gate_weight[0].T,
        up_weight[0].T,
        down_weight[0],
    )
    piece = width // PIECES
    expert_output, attention_output = pl.pallas_call(
        blend_kernel,
        grid=(PIECES,),
        out_shape=(
            jax.ShapeDtypeStruct((tokens, width), BF16),
            jax.ShapeDtypeStruct((rows // (2 * NZ), width), BF16),
        ),
        in_specs=[
            pl.BlockSpec(blend.shape, lambda i: (0, 0, 0)),
            pl.BlockSpec((EP * CAP, piece), lambda i: (0, i)),
            pl.BlockSpec(attn.shape, lambda i: (0, 0, 0)),
        ],
        out_specs=(
            pl.BlockSpec((tokens, piece), lambda i: (0, i)),
            pl.BlockSpec((rows // (2 * NZ), width), lambda i: (0, 0)),
        ),
    )(blend, returned.reshape(EP * CAP, width), attn)
    return attention_output, expert_output


def solution(mesh):
    in_specs = (
        P("ep", "tp"),
        P("ep", "tp"),
        P("ep", "tp"),
        P(),
        P(),
        P("tp"),
        P("tp", None),
        P(("ep", "tp"), None),
        P(),
        P(("ep", "tp"), None),
        P(("ep", "tp"), None),
        P("ep", None, "tp"),
        P("ep", None, "tp"),
        P("ep", "tp", None),
    )
    out_specs = (P(("ep", "tp"), None), P(("ep", "tp"), None))
    return jax.shard_map(body, mesh=mesh, in_specs=in_specs, out_specs=out_specs, check_vma=False)
```

```python
import functools

import jax
import jax.numpy as jnp
from jax import lax
from jax.experimental import pallas as pl
from jax.experimental.pallas import tpu as pltpu
from jax.sharding import PartitionSpec as P

HEAD_DIM = 64
EPS = 1e-06
MESH = pl.DeviceIdType.MESH
EP = 16
NZ = 8
CAP = 16
HALF = EP // 2
PIECES = 2
CHUNKS = 8
F32 = jnp.float32
BF16 = jnp.bfloat16


def iota(shape, dim):
    return lax.broadcasted_iota(jnp.int32, shape, dim)


def kernel(
    query_hbm,
    key_hbm,
    value_hbm,
    query_gain_hbm,
    key_gain_hbm,
    offset_hbm,
    mixer_hbm,
    tokens_hbm,
    expert_gain_hbm,
    routes_hbm,
    scores_hbm,
    gate_hbm,
    up_hbm,
    down_hbm,
    attn_hbm,
    blend_hbm,
    returned,
    query_ref,
    key_ref,
    value_ref,
    query_gain_ref,
    key_gain_ref,
    offset_ref,
    tokens_ref,
    expert_gain_ref,
    routes_ref,
    scores_ref,
    gate_w,
    up_w,
    down_w,
    mixer_w,
    kv,
    tok,
    slots,
    outgoing,
    arrived,
    terms,
    ring_out,
    ring_in,
    blend,
    mix_mine,
    mix_theirs,
    mix_terms,
    mix_out,
    mix_in,
    load_sem,
    small_sem,
    pair_send,
    pair_recv,
    kv_send,
    kv_recv,
    ag_send,
    up_recv,
    dn_recv,
    slot_send,
    slot_recv,
    disp_send,
    disp_recv,
    ring_send,
    ring_recv,
    ret_send,
    ret_recv,
    mix_send,
    mix_recv,
):
    ep = lax.axis_index("ep")
    tp = lax.axis_index("tp")
    z, core = tp // 2, tp % 2
    above = (ep, lax.rem(z + 1, NZ) * 2 + core)
    below = (ep, lax.rem(z + NZ - 1, NZ) * 2 + core)
    sibling = (ep, z * 2 + 1 - core)
    rows = query_hbm.shape[0]
    tokens, width = tokens_hbm.shape
    position_here = lax.rem(ep // 4 + ep % 4, 4) * 4 + ep // 4
    goes_up = position_here < HALF

    def at_position(place):
        return place % 4 * 4 + lax.rem(place // 4 + 4 - place % 4, 4)

    def remote(src, dst, send, recv, device):
        return pltpu.make_async_remote_copy(
            src_ref=src,
            dst_ref=dst,
            send_sem=send,
            recv_sem=recv,
            device_id=device,
            device_id_type=MESH,
        )

    barrier = pltpu.get_barrier_semaphore()

    greeted = [(ep, lax.rem(z + j, NZ) * 2 + core) for j in range(1, NZ)]
    greeted += [(lax.rem(ep + j, EP), tp) for j in range(1, EP)] + [sibling]
    for peer in greeted:
        pl.semaphore_signal(barrier, inc=1, device_id=peer, device_id_type=MESH)

    operands = (
        (tokens_hbm, tokens_ref),
        (expert_gain_hbm, expert_gain_ref),
        (routes_hbm, routes_ref),
        (key_hbm, key_ref),
        (value_hbm, value_ref),
        (key_gain_hbm, key_gain_ref),
        (query_hbm, query_ref),
        (query_gain_hbm, query_gain_ref),
        (offset_hbm, offset_ref),
        (scores_hbm, scores_ref),
    )
    small = [
        pltpu.make_async_copy(src, dst, small_sem.at[i]) for i, (src, dst) in enumerate(operands)
    ]
    for copy in small:
        copy.start()

    weights = ((gate_hbm, gate_w), (up_hbm, up_w), (down_hbm, down_w), (mixer_hbm, mixer_w))
    loads = [
        pltpu.make_async_copy(src, dst.at[0], load_sem.at[i])
        for i, (src, dst) in enumerate(weights)
    ]
    for copy in loads:
        copy.start()

    lane = iota((rows, 128), 1)
    first_head = lane < HEAD_DIM

    def norm_heads(flat, gain):
        split = flat.astype(F32)
        squares = split * split
        mean_a = jnp.sum(jnp.where(first_head, squares, 0.0), axis=1, keepdims=True) / HEAD_DIM
        mean_b = jnp.sum(jnp.where(first_head, 0.0, squares), axis=1, keepdims=True) / HEAD_DIM
        scale = jnp.where(first_head, lax.rsqrt(mean_a + EPS), lax.rsqrt(mean_b + EPS))
        return (split * scale * jnp.concatenate([gain, gain], axis=1)).astype(BF16)

    for copy in small[:3]:
        copy.wait()
    as_float = tokens_ref[...].astype(F32)
    mean = jnp.mean(as_float * as_float, axis=1, keepdims=True)
    tok[0] = (as_float * lax.rsqrt(mean + EPS) * expert_gain_ref[...]).astype(BF16)

    expert_row = iota((EP, tokens), 0)
    member_a = jnp.where(routes_ref[0:1, :] == expert_row, 1.0, 0.0).astype(F32)
    member_b = jnp.where(routes_ref[1:2, :] == expert_row, 1.0, 0.0).astype(F32)
    earlier = jnp.where(iota((tokens, tokens), 0) < iota((tokens, tokens), 1), 1.0, 0.0)
    earlier = earlier.astype(BF16)
    ahead_a = jnp.dot(member_a.astype(BF16), earlier, preferred_element_type=F32)
    ahead_b = jnp.dot(member_b.astype(BF16), earlier, preferred_element_type=F32)
    ahead_b = ahead_b + jnp.sum(member_a, axis=1, keepdims=True)
    expert_base = (expert_row * CAP).astype(F32)
    slot_a = jnp.sum(member_a * (ahead_a + expert_base), axis=0, keepdims=True)
    slot_b = jnp.sum(member_b * (ahead_b + expert_base), axis=0, keepdims=True)
    slots[0, 0] = jnp.broadcast_to(slot_a, (8, tokens))
    slots[0, 1] = jnp.broadcast_to(slot_b, (8, tokens))

    with jax.named_scope("wait_entry"):
        pl.semaphore_wait(barrier, len(greeted))

    part_tok = tokens // 2

    def ag_up(hop, chunk):
        part = pl.ds(chunk * part_tok, part_tok)
        return remote(
            tok.at[hop - 1, part],
            tok.at[hop, part],
            ag_send,
            up_recv.at[chunk, hop],
            above,
        )

    def ag_down(hop, chunk):
        part = pl.ds(chunk * part_tok, part_tok)
        return remote(
            tok.at[lax.rem(NZ + 1 - hop, NZ), part],
            tok.at[NZ - hop, part],
            ag_send,
            dn_recv.at[chunk, hop],
            below,
        )

    def slot_copy(j):
        peer = (ep, lax.rem(z + j, NZ) * 2 + core)
        return remote(slots.at[0], slots.at[j], slot_send, slot_recv.at[j], peer)

    def send_slots(j, _):
        slot_copy(j).start()
        return 0

    lax.fori_loop(1, NZ, send_slots, 0)
    for chunk in range(2):
        ag_up(1, chunk).start()
        ag_down(1, 1 - chunk).start()

    for copy in small[3:]:
        copy.wait()
    key_norm = norm_heads(key_ref[...], key_gain_ref[...])
    kv[ep, 0] = key_norm
    kv[ep, 1] = value_ref[...]

    def kv_copy(source, target):
        return remote(
            kv.at[source], kv.at[source], kv_send.at[target], kv_recv.at[source], (target, tp)
        )

    def send_kv(j, _):
        kv_copy(ep, j).start()
        return 0

    lax.fori_loop(ep + 1, EP, send_kv, 0)

    pair_copies = [
        remote(src, dst.at[1], pair_send.at[i], pair_recv.at[i], sibling)
        for i, (src, dst) in enumerate(weights)
    ]
    for copy in pair_copies:
        copy.start()

    slot_rows = iota((EP * CAP, tokens), 0).astype(F32)

    def dispatch(step, distance):
        row_a = slots[distance, 0][0:1]
        row_b = slots[distance, 1][0:1]
        pick = jnp.where((slot_rows == row_a) | (slot_rows == row_b), 1.0, 0.0).astype(BF16)
        picked = jnp.dot(pick, tok[distance], preferred_element_type=F32).astype(BF16)
        outgoing[pl.ds(step * EP, EP)] = picked.reshape(EP, CAP, width)

        def send(j, _):
            peer = lax.rem(ep // 4 + j // 4, 4) * 4 + lax.rem(ep % 4 + j % 4, 4)
            remote(
                outgoing.at[step * EP + peer],
                arrived.at[step, position_here],
                disp_send,
                disp_recv.at[step],
                (peer, tp),
            ).start()
            return 0

        lax.fori_loop(1, EP, send, 0)
        arrived[step, position_here] = outgoing[step * EP + ep]

    def all_but_one(buffer, send, recv):
        block = buffer.at[pl.ds(0, EP - 1)]
        return remote(block, block, send, recv, sibling)

    def wait_slots(j, _):
        slot_copy(j).wait_recv()
        return 0

    def advance(step):
        @pl.when(step <= 3)
        def _():
            for chunk in range(2):
                with jax.named_scope("wait_up"):
                    ag_up(step, chunk).wait_recv()

                @pl.when(step <= 3 - chunk)
                def _():
                    ag_up(step + 1, chunk).start()

                with jax.named_scope("wait_down"):
                    ag_down(step, 1 - chunk).wait_recv()

                @pl.when(step <= 3 - chunk)
                def _():
                    ag_down(step + 1, 1 - chunk).start()

        @pl.when(step == 4)
        def _():
            with jax.named_scope("wait_last"):
                ag_up(4, 0).wait_recv()
                ag_down(4, 1).wait_recv()

        @pl.when(step == 1)
        def _():
            with jax.named_scope("wait_slots"):
                lax.fori_loop(1, NZ, wait_slots, 0)

        with jax.named_scope("dispatch"):
            distance = lax.rem(jnp.where(goes_up, step, NZ - step), NZ)
            dispatch(lax.rem(step, NZ), distance)

    def attention():
        query_norm = norm_heads(query_ref[...], query_gain_ref[...])
        zero = jnp.zeros_like(query_norm)
        queries = jnp.concatenate(
            [jnp.where(first_head, query_norm, zero), jnp.where(first_head, zero, query_norm)],
            axis=0,
        )
        row = iota((2 * rows, rows), 0)
        column = iota((2 * rows, rows), 1)
        offsets = jnp.where(row < rows, offset_ref[0], offset_ref[1])
        position = jnp.where(row < rows, row, row - rows)
        after = jnp.where(iota((rows, rows), 0) > iota((rows, rows), 1), 1.0, 0.0).astype(BF16)

        def absorb(j, state):
            mixed, carried = state

            @pl.when(j < ep)
            def _():
                kv_copy(j, ep).wait_recv()

            keys, values = kv[j, 0], kv[j, 1]
            scores = lax.dot_general(
                queries, keys, (((1,), (1,)), ((), ())), preferred_element_type=F32
            )
            scores = scores * HEAD_DIM ** (-0.5) + offsets
            allowed = (column < position) | (j < ep)
            log_fail = -(jnp.maximum(scores, 0.0) + jnp.log1p(jnp.exp(-jnp.abs(scores))))
            log_rise = scores + log_fail
            log_fail = jnp.where(allowed, log_fail, 0.0)
            high = log_fail.astype(BF16)
            rest = log_fail - high.astype(F32)
            middle = rest.astype(BF16)
            low = (rest - middle.astype(F32)).astype(BF16)
            between = (
                jnp.dot(high, after, preferred_element_type=F32)
                + jnp.dot(middle, after, preferred_element_type=F32)
                + jnp.dot(low, after, preferred_element_type=F32)
            )
            weights = jnp.where(allowed, jnp.exp(log_rise + between + carried), 0.0).astype(BF16)
            mixed = mixed + jnp.dot(weights, values, preferred_element_type=F32)
            carried = carried + jnp.sum(log_fail, axis=1, keepdims=True)
            return mixed, carried

        state = (jnp.zeros((2 * rows, 128), F32), jnp.zeros((2 * rows, 1), F32))
        mixed, _ = lax.fori_loop(0, ep + 1, lambda t, s: absorb(ep - t, s), state)
        heads = jnp.where(first_head, mixed[:rows], mixed[rows:]).astype(BF16)
        to_row = iota((rows, rows), 0)
        from_row = iota((rows, rows), 1)
        owner_core = to_row // 64
        within = to_row % 64
        source = (within // 8) * 16 + owner_core * 8 + within % 8
        order = jnp.where(from_row == source, 1.0, 0.0).astype(BF16)
        ordered = jnp.dot(order, heads, preferred_element_type=F32).astype(BF16)
        mix_mine[0] = ordered[:64]
        mix_mine[1] = ordered[64:]

    def mix_pair():
        return remote(
            mix_mine.at[1 - core], mix_theirs, pair_send.at[4], pair_recv.at[4], sibling
        )

    def project():
        loads[3].wait()
        pair_copies[3].wait_recv()
        mix_pair().wait_recv()
        term = jnp.dot(mix_mine[core], mixer_w[0], preferred_element_type=F32)
        term = term + jnp.dot(mix_theirs[...], mixer_w[1], preferred_element_type=F32)
        for i in range(NZ):
            for part in range(2):
                columns = slice(part * width // 2, (part + 1) * width // 2)
                mix_terms[i, part] = term[8 * i : 8 * i + 8, columns]

    def mix_ring(step, part):
        return remote(
            mix_out.at[step, part],
            mix_in.at[step + 1, part],
            mix_send,
            mix_recv.at[part, step + 1],
            (above, below)[part],
        )

    def mix(step):
        for part, owner in ((0, z + NZ - step), (1, z + step)):
            mine = mix_terms[lax.rem(owner, NZ), part]

            @pl.when(step == 1)
            def _():
                mix_out[step, part] = mine.astype(BF16)

            @pl.when(step >= 2)
            def _():
                with jax.named_scope("wait_mix"):
                    mix_ring(step - 1, part).wait_recv()
                mix_out[step, part] = (mine + mix_in[step, part].astype(F32)).astype(BF16)

            @pl.when(step < NZ)
            def _():
                mix_ring(step, part).start()

    def experts(step):
        rows_in = arrived[lax.rem(step, NZ)].reshape(EP * CAP, width)
        across = (((1,), (1,)), ((), ()))
        units = 2 * gate_w.shape[1]
        gate = lax.dot_general(
            rows_in, gate_w[...].reshape(units, width), across, preferred_element_type=F32
        )
        up = lax.dot_general(
            rows_in, up_w[...].reshape(units, width), across, preferred_element_type=F32
        )
        hidden = (gate / (1.0 + jnp.exp(-gate)) * up).astype(BF16)
        terms[...] = jnp.dot(
            hidden, down_w[...].reshape(units, width), preferred_element_type=F32
        )

    share = width // CHUNKS

    def ring(step, part, chunk):
        block = (pl.ds(part * HALF, HALF), slice(None), pl.ds(chunk * share, share))
        return remote(
            ring_out.at[step, *block],
            ring_in.at[step - 1, *block],
            ring_send,
            ring_recv.at[part * CHUNKS + chunk, step - 1],
            (above, below)[part],
        )

    def combine(step):
        for chunk in range(CHUNKS):
            columns = slice(chunk * share, (chunk + 1) * share)
            for part in range(2):
                blocks = pl.ds(part * HALF, HALF)
                mine = terms[part * HALF * CAP : (part + 1) * HALF * CAP, columns]

                @pl.when(step == 1)
                def _():
                    ring_out[step, blocks, :, columns] = mine.astype(BF16).reshape(HALF, CAP, share)

                @pl.when(step >= 2)
                def _():
                    with jax.named_scope("wait_ring"):
                        ring(step - 1, part, chunk).wait_recv()
                    sofar = ring_in[step - 2, blocks, :, columns].reshape(HALF * CAP, share)
                    total = (mine + sofar.astype(F32)).astype(BF16)
                    ring_out[step, blocks, :, columns] = total.reshape(HALF, CAP, share)

                @pl.when(step < NZ)
                def _():
                    ring(step, part, chunk).start()

                @pl.when(step == NZ)
                def _():
                    def send(j, _):
                        place = part * HALF + lax.rem(position_here + j, HALF)
                        peer = at_position(place)

                        @pl.when(peer != ep)
                        def _():
                            remote(
                                ring_out.at[NZ, place, :, pl.ds(chunk * share, share)],
                                returned.at[ep, :, pl.ds(chunk * share, share)],
                                ret_send,
                                ret_recv,
                                (peer, tp),
                            ).start()

                        return 0

                    lax.fori_loop(0, HALF, send, 0)

    advance(1)
    advance(2)
    with jax.named_scope("attention"):
        attention()
    mix_pair().start()
    for i in range(3):
        loads[i].wait()
        pair_copies[i].wait_recv()

    def one_step(step, _):
        every = all_but_one(
            arrived.at[lax.rem(step, NZ)], disp_send, disp_recv.at[lax.rem(step, NZ)]
        )
        with jax.named_scope("wait_arrived"):
            every.wait_recv()
        with jax.named_scope("experts"):
            experts(step)

        @pl.when(step <= 2)
        def _():
            advance(step + 2)

        combine(step)

        @pl.when((step >= 2) & (step + 3 <= NZ))
        def _():
            advance(step + 3)

        @pl.when(step == 1)
        def _():
            with jax.named_scope("mixer"):
                project()

        mix(step)

        return 0

    lax.fori_loop(1, NZ + 1, one_step, 0)
    own = pltpu.make_async_copy(ring_out.at[NZ, position_here], returned.at[ep], load_sem.at[4])
    own.start()
    attn_copy = pltpu.make_async_copy(mix_out.at[NZ], attn_hbm, load_sem.at[6])
    attn_copy.start()

    def column(row):
        return jnp.transpose(jnp.broadcast_to(row, (tokens, tokens)))[:, 0:1]

    slot_lane = iota((tokens, EP * CAP), 1).astype(F32)
    score_a, score_b = scores_ref[0:1, :], scores_ref[1:2, :]
    weight_a = column(1.0 / (1.0 + jnp.exp(score_b - score_a)))
    weight_b = column(1.0 / (jnp.exp(score_a - score_b) + 1.0))
    weight = jnp.where(slot_lane == column(slots[0, 0][0:1]), weight_a, 0.0)
    weight = jnp.where(slot_lane == column(slots[0, 1][0:1]), weight_b, weight)
    high = weight.astype(BF16)
    blend[0] = high
    blend[1] = (weight - high.astype(F32)).astype(BF16)
    blend_copy = pltpu.make_async_copy(blend, blend_hbm, load_sem.at[5])
    blend_copy.start()

    mix_pair().wait_send()
    for copy in pair_copies:
        copy.wait_send()

    def drain(block, send, recv):
        remote(block, block, send, recv, sibling).wait_send()

    drain(tok.at[pl.ds(0, NZ - 1)], ag_send, up_recv.at[0, 0])
    drain(slots.at[pl.ds(1, NZ - 1)], slot_send, slot_recv.at[0])
    drain(outgoing.at[pl.ds(0, NZ * (EP - 1))], disp_send, disp_recv.at[0])
    drain(mix_out.at[pl.ds(1, NZ - 1)], mix_send, mix_recv.at[0, 0])
    drain(ring_out.at[pl.ds(1, NZ - 1)], ring_send, ring_recv.at[0, 0])

    def drain_kv(j, _):
        kv_copy(ep, j).wait_send()
        return 0

    lax.fori_loop(ep + 1, EP, drain_kv, 0)

    with jax.named_scope("wait_returned"):
        own.wait()
        blend_copy.wait()
        all_but_one(returned, ret_send, ret_recv).wait()
        attn_copy.wait()


def blend_kernel(blend_ref, results_ref, attn_ref, expert_out, attn_out):
    _, tokens, slots = blend_ref.shape
    parts = jnp.dot(
        blend_ref[...].reshape(2 * tokens, slots), results_ref[...], preferred_element_type=F32
    )
    expert_out[...] = (parts[:tokens] + parts[tokens:]).astype(BF16)

    @pl.when(pl.program_id(0) == 0)
    def _():
        half = attn_ref.shape[2]
        attn_out[:, :half] = attn_ref[0]
        attn_out[:, half:] = attn_ref[1]


def body(
    query_rows,
    key_rows,
    value_rows,
    query_norm_gain,
    key_gain,
    break_offset,
    mixer_out_weight,
    routed_tokens,
    expert_gain,
    routes,
    route_scores,
    gate_weight,
    up_weight,
    down_weight,
):
    rows = query_rows.shape[0]
    tokens, width = routed_tokens.shape
    units = gate_weight.shape[2]
    hbm = pl.BlockSpec(memory_space=pl.ANY)
    dma = pltpu.SemaphoreType.DMA
    attn, blend, returned = pl.pallas_call(
        kernel,
        out_shape=(
            jax.ShapeDtypeStruct((2, rows // (2 * NZ), width // 2), BF16),
            jax.ShapeDtypeStruct((2, tokens, EP * CAP), BF16),
            jax.ShapeDtypeStruct((EP, CAP, width), BF16),
        ),
        in_specs=[hbm] * 14,
        out_specs=(hbm, hbm, hbm),
        scratch_shapes=[
            pltpu.VMEM((rows, 128), BF16),
            pltpu.VMEM((rows, 128), BF16),
            pltpu.VMEM((rows, 128), BF16),
            pltpu.VMEM((1, HEAD_DIM), F32),
            pltpu.VMEM((1, HEAD_DIM), F32),
            pltpu.SMEM((2,), F32),
            pltpu.VMEM((tokens, width), BF16),
            pltpu.VMEM((1, width), F32),
            pltpu.VMEM((2, tokens), jnp.int32),
            pltpu.VMEM((2, tokens), F32),
            pltpu.VMEM((2, units, width), BF16),
            pltpu.VMEM((2, units, width), BF16),
            pltpu.VMEM((2, units, width), BF16),
            pltpu.VMEM((2, 128, width), BF16),
            pltpu.VMEM((EP, 2, rows, 128), BF16),
            pltpu.VMEM((NZ, tokens, width), BF16),
            pltpu.VMEM((NZ, 2, 8, 128), F32),
            pltpu.VMEM((NZ * EP, CAP, width), BF16),
            pltpu.VMEM((NZ, EP, CAP, width), BF16),
            pltpu.VMEM((EP * CAP, width), F32),
            pltpu.VMEM((NZ + 1, EP, CAP, width), BF16),
            pltpu.VMEM((NZ - 1, EP, CAP, width), BF16),
            pltpu.VMEM((2, tokens, EP * CAP), BF16),
            pltpu.VMEM((2, 64, 128), BF16),
            pltpu.VMEM((64, 128), BF16),
            pltpu.VMEM((NZ, 2, 8, width // 2), F32),
            pltpu.VMEM((NZ + 1, 2, 8, width // 2), BF16),
            pltpu.VMEM((NZ + 1, 2, 8, width // 2), BF16),
            dma((7,)),
            dma((10,)),
            dma((5,)),
            dma((5,)),
            dma((EP,)),
            dma((EP,)),
            dma,
            dma((2, 5)),
            dma((2, 5)),
            dma,
            dma((NZ,)),
            dma,
            dma((NZ,)),
            dma,
            dma((2 * CHUNKS, NZ - 1)),
            dma,
            dma,
            dma,
            dma((2, NZ + 1)),
        ],
        compiler_params=pltpu.CompilerParams(
            collective_id=0, has_side_effects=True, vmem_limit_bytes=67043328
        ),
    )(
        query_rows,
        key_rows,
        value_rows,
        query_norm_gain[None, :],
        key_gain[None, :],
        break_offset,
        mixer_out_weight,
        routed_tokens,
        expert_gain[None, :],
        routes.T,
        route_scores.T,
        gate_weight[0].T,
        up_weight[0].T,
        down_weight[0],
    )
    piece = width // PIECES
    expert_output, attention_output = pl.pallas_call(
        blend_kernel,
        grid=(PIECES,),
        out_shape=(
            jax.ShapeDtypeStruct((tokens, width), BF16),
            jax.ShapeDtypeStruct((rows // (2 * NZ), width), BF16),
        ),
        in_specs=[
            pl.BlockSpec(blend.shape, lambda i: (0, 0, 0)),
            pl.BlockSpec((EP * CAP, piece), lambda i: (0, i)),
            pl.BlockSpec(attn.shape, lambda i: (0, 0, 0)),
        ],
        out_specs=(
            pl.BlockSpec((tokens, piece), lambda i: (0, i)),
            pl.BlockSpec((rows // (2 * NZ), width), lambda i: (0, 0)),
        ),
    )(blend, returned.reshape(EP * CAP, width), attn)
    return attention_output, expert_output


def solution(mesh):
    in_specs = (
        P("ep", "tp"),
        P("ep", "tp"),
        P("ep", "tp"),
        P(),
        P(),
        P("tp"),
        P("tp", None),
        P(("ep", "tp"), None),
        P(),
        P(("ep", "tp"), None),
        P(("ep", "tp"), None),
        P("ep", None, "tp"),
        P("ep", None, "tp"),
        P("ep", "tp", None),
    )
    out_specs = (P(("ep", "tp"), None), P(("ep", "tp"), None))
    return jax.shard_map(body, mesh=mesh, in_specs=in_specs, out_specs=out_specs, check_vma=False)
```
